32 devices in a mesh: dp: 4 (over y, x), kv: 4 (over z), tp: 2 (over core).
Axes of the slice: x: 2, y: 2, z: 4, core: 2. Of those that a mesh axis runs over, the one named last changes fastest.
Arguments:
- tokens: bfloat16 [256, 2048], P('dp', ('kv', 'tp')), parts along dimension 0, may hold values from -64 to 64, as said below
- lengths: int32 [32], P(('dp', 'kv', 'tp')), parts along dimension 0, may hold values from 1 to 8, 28 in all
- state: float32 [32, 16, 128, 128], P(('dp', 'kv', 'tp')), parts along dimension 0, may hold values from -1.8 to 1.8
- gain_first: float32 [2048], replicated, may hold values from 0.1 to 1.9
- first_gate: bfloat16 [2048, 5632], P(None, 'kv'), may hold values from -0.125 to 0.125
- first_up: bfloat16 [2048, 5632], P(None, 'kv'), may hold values from -0.125 to 0.125
- first_down: bfloat16 [5632, 2048], P('kv'), may hold values from -0.109375 to 0.109375
- gain_mix: float32 [2048], replicated, may hold values from 0.1 to 1.9
- query_weight: bfloat16 [2048, 2048], P(None, ('kv', 'tp')), may hold values from -0.125 to 0.125
- key_weight: bfloat16 [2048, 2048], P(None, ('kv', 'tp')), may hold values from -0.125 to 0.125
- value_weight: bfloat16 [2048, 2048], P(None, ('kv', 'tp')), may hold values from -0.125 to 0.125
- gating_weight: bfloat16 [2048, 2048], P(None, ('kv', 'tp')), may hold values from -0.125 to 0.125
- write_weight: bfloat16 [2048, 16], replicated, may hold values from -0.125 to 0.125
- forget_weight: bfloat16 [2048, 16], replicated, may hold values from -0.125 to 0.125
- forget_rate: float32 [16], replicated, may hold values from -4 to 1.5
- out_weight: bfloat16 [2048, 2048], P(None, ('kv', 'tp')), may hold values from -0.125 to 0.125
- gain_second: float32 [2048], replicated, may hold values from 0.1 to 1.9
- second_gate: bfloat16 [2048, 5632], P(None, 'kv'), may hold values from -0.125 to 0.125
- second_up: bfloat16 [2048, 5632], P(None, 'kv'), may hold values from -0.125 to 0.125
- second_down: bfloat16 [5632, 2048], P('kv'), may hold values from -0.109375 to 0.109375
Outputs:
- mixed_out: bfloat16 [256, 2048], P('dp', ('kv', 'tp')), parts along dimension 0
- new_state: float32 [32, 16, 128, 128], P(('dp', 'kv', 'tp')), parts along dimension 0
The draws below stay inside these ranges and needn't reach their ends.
There are 4 independent parts, one for each index of `dp`. The reference program is written for one: setup_inputs(seed, part) draws one part's arguments, and reference() takes and returns one part's arrays. A program takes and returns all parts, laid end to end along the dimension named above; an argument that names none is the same for every part. Nothing has to cross between parts.
Inputs may be any that keep to these rules, and one draw needn't show every extreme that they name: Activations of the new tokens. `lengths`: the live new tokens of each sequence; within each independent group of 8 sequences (one part along dp) they sum to seven halves of 8, rounded down, and some sequence of each group has all 8 live.
All inputs are finite; a program needn't handle non-finite values.
Results may differ from the reference program's by a relative error of at most 0.0058.
Values may be sent and summed in bfloat16 or wider, within the bound.
A program may use at most 128 MiB of HBM per device.

```python
import math
import jax
import jax.numpy as jnp
import numpy as np
from jax import lax

D = 2048
HEADS = 16
HEAD = 128
FF = 5632
BLK = 8
SEQS = 8
ROWS = 64


def draw_tokens(key, part):
    key_base = jax.random.fold_in(key, 17)
    key_one, key_two, key_three = jax.random.split(key_base, 3)
    columns = jnp.arange(D, dtype=jnp.float32)
    rough_cols = jnp.exp(jax.random.uniform(key_two, (1, D), jnp.float32, -0.35, 0.35))
    col_scale = jnp.exp(math.log(5.0) * (columns[None, :] / D - 0.5)) * rough_cols
    base = jnp.clip(jax.random.normal(key_one, (ROWS, D), jnp.float32), -5.0, 5.0)
    row_scale = jnp.exp(jax.random.uniform(key_three, (ROWS, 1), jnp.float32, math.log(0.4), math.log(4.0)))
    return (base * row_scale * col_scale).astype(jnp.bfloat16)


def spiked(array, key, source, target, blocks, factor):
    owner, partner = [(jnp.arange(array.shape[position]) // (array.shape[position] // blocks)).reshape([-1 if axis == position else 1 for axis in range(array.ndim)]) for position in (source, target)]
    chosen = jax.random.permutation(key, blocks)[partner]
    strong = (owner == chosen) | (owner == (partner + blocks // 2) % blocks)
    return jnp.where(strong, factor * array, array)


def steps_of(own_key, dims, pieces, smallest, high):
    level = 1.0
    for axis_at, parts in pieces:
        heights = jax.random.uniform(jax.random.fold_in(jax.random.fold_in(own_key, 6), axis_at), (parts,), jnp.float32, smallest / len(pieces), high / len(pieces))
        level = level * jnp.repeat(jnp.exp(heights), dims[axis_at] // parts).reshape((-1,) + (1,) * (len(dims) - 1 - axis_at))
    return level


def profile(count, total, most, skew):
    loads = [(1 << 20) // math.isqrt(standing ** skew) + 1 for standing in range(2, count + 1)]
    spare, given = total - most - (count - 1), [1] * (count - 1)
    while spare > 0:
        free = [i for i in range(count - 1) if given[i] < most]
        whole, left = sum([loads[i] for i in free]), spare
        for i in free:
            addition = min(most - given[i], max(1, left * loads[i] // whole), spare)
            given[i] = given[i] + addition
            spare = spare - addition
    return np.array([most] + given)


def uneven_parts(stream_key, number_of, total, most, slope):
    if number_of == 2:
        one = jax.random.randint(stream_key, (), max(1, total - most), min(most, total - 1) + 1)
        return jnp.stack([one, total - one])
    tallies = jnp.asarray(profile(number_of, total, most, slope), jnp.int32)
    pairs = (number_of - 1) // 2
    source_of, taker = tallies[1:1 + 2 * pairs:2], tallies[2:2 + 2 * pairs:2]
    slack = jnp.minimum(source_of - 1, most - taker)
    passed = jax.random.randint(jax.random.fold_in(stream_key, 1), (pairs,), 0, 1 << 20) % (slack + 1)
    tallies = tallies.at[1:1 + 2 * pairs:2].set(source_of - passed).at[2:2 + 2 * pairs:2].set(taker + passed)
    return tallies[jax.random.permutation(jax.random.fold_in(stream_key, 2), number_of)]


def gaussian(own_key, extent, spread, most, shards=(), kind=jnp.bfloat16):
    loudness = steps_of(own_key, extent, shards, -0.22, 0.18) if shards else 1.0
    values = jax.random.normal(own_key, extent, jnp.float32) * spread * loudness
    return jnp.minimum(jnp.maximum(values, -most), most).astype(kind)


def gaussian_with(stream_key, shape, scale, most, cuts, heavy, held_as=jnp.bfloat16):
    values = scale * jax.random.normal(stream_key, shape, jnp.float32)
    if cuts:
        values = values * steps_of(stream_key, shape, cuts, -0.22, 0.18)
    return jnp.clip(spiked(values, jax.random.fold_in(stream_key, 3), *heavy), -most, most).astype(held_as)


def setup_inputs(seed: int = 0, part: int = 0) -> dict:
    keys = jax.random.split(jax.random.key(seed), 21)
    part_splits = jax.random.split(jax.random.fold_in(keys[20], part), 21)
    tokens = draw_tokens(jax.random.fold_in(jax.random.fold_in(keys[20], part), 71), part)
    lengths = uneven_parts(part_splits[1], SEQS, SEQS * 7 // 2, BLK, 2).astype(jnp.int32)
    state = gaussian(part_splits[2], (SEQS, HEADS, HEAD, HEAD), 0.3, 1.8, ((0, 8),), jnp.float32)
    gain_first = jnp.clip(1.0 + 0.18 * jax.random.normal(keys[3], (D,), jnp.float32), 0.1, 1.9)
    first_gate = gaussian(keys[4], (D, FF), D ** -0.5, 0.125, ((1, 4),))
    first_up = gaussian(keys[5], (D, FF), D ** -0.5, 0.125, ((1, 4),))
    first_down = gaussian_with(keys[6], (FF, D), FF ** -0.5, 0.109375, ((0, 4),), (0, 1, 4, 2.0))
    gain_mix = jnp.clip(1.0 + 0.18 * jax.random.normal(keys[7], (D,), jnp.float32), 0.1, 1.9)
    query_weight = gaussian(keys[8], (D, HEADS * HEAD), D ** -0.5, 0.125, ((1, 8),))
    key_weight = gaussian(keys[9], (D, HEADS * HEAD), D ** -0.5, 0.125, ((1, 8),))
    value_weight = gaussian(keys[10], (D, HEADS * HEAD), D ** -0.5, 0.125, ((1, 8),))
    gating_weight = gaussian(keys[11], (D, HEADS * HEAD), D ** -0.5, 0.125, ((1, 8),))
    write_weight = gaussian(keys[12], (D, HEADS), D ** -0.5, 0.125)
    forget_weight = gaussian(keys[13], (D, HEADS), D ** -0.5, 0.125)
    forget_rate = jnp.clip(jax.random.uniform(keys[14], (HEADS,), jnp.float32, -4.0, 1.5), -4.0, 1.5)
    out_weight = gaussian(keys[15], (HEADS * HEAD, D), (HEADS * HEAD) ** -0.5, 0.125, ((1, 8),))
    gain_second = jnp.clip(1.0 + 0.18 * jax.random.normal(keys[16], (D,), jnp.float32), 0.1, 1.9)
    second_gate = gaussian(keys[17], (D, FF), D ** -0.5, 0.125, ((1, 4),))
    second_up = gaussian(keys[18], (D, FF), D ** -0.5, 0.125, ((1, 4),))
    second_down = gaussian_with(keys[19], (FF, D), FF ** -0.5, 0.109375, ((0, 4),), (0, 1, 4, 2.0))
    return {"tokens": tokens, "lengths": lengths, "state": state, "gain_first": gain_first, "first_gate": first_gate, "first_up": first_up, "first_down": first_down, "gain_mix": gain_mix, "query_weight": query_weight, "key_weight": key_weight, "value_weight": value_weight, "gating_weight": gating_weight, "write_weight": write_weight, "forget_weight": forget_weight, "forget_rate": forget_rate, "out_weight": out_weight, "gain_second": gain_second, "second_gate": second_gate, "second_up": second_up, "second_down": second_down}


EPSILON = 1e-06

def feed_forward(hidden_in, gain, w_gate, w_up, w_down):
    values = hidden_in.astype(jnp.float32)
    row_scale = lax.rsqrt(lax.optimization_barrier(jnp.mean(values * values, axis=1, keepdims=True)) + EPSILON)
    scaled = (values * gain).astype(jnp.bfloat16)
    gate_act = jnp.dot(scaled, w_gate, preferred_element_type=jnp.float32) * row_scale
    up_act = jnp.dot(scaled, w_up, preferred_element_type=jnp.float32) * row_scale
    hidden = (jax.nn.silu(gate_act) * up_act).astype(jnp.bfloat16)
    result = jnp.dot(hidden, w_down, preferred_element_type=jnp.float32)
    return (values + 0.5 * result).astype(jnp.bfloat16)

def delta_block(query, key_in, value, gating, write_pre, forget_pre, rates, live, state):
    seq_count, block_len, head_count, head_size = query.shape
    precise = lax.Precision.HIGHEST
    query_unit = query * lax.rsqrt(lax.optimization_barrier(jnp.sum(query * query, axis=-1, keepdims=True)) + EPSILON) / math.sqrt(head_size)
    key_unit = key_in * lax.rsqrt(lax.optimization_barrier(jnp.sum(key_in * key_in, axis=-1, keepdims=True)) + EPSILON)
    live_rows = live[:, :, None]
    write_gate = jax.nn.sigmoid(write_pre) * live_rows
    forget = -jnp.exp(rates)[None, None, :] * jax.nn.softplus(forget_pre) * live_rows
    cumulative = jnp.cumsum(forget, axis=1)
    cum_heads = jnp.transpose(cumulative, (0, 2, 1))
    positions = jnp.arange(block_len)
    causal = positions[:, None] >= positions[None, :]
    strict = positions[:, None] > positions[None, :]
    differ = jnp.minimum(cum_heads[:, :, :, None] - cum_heads[:, :, None, :], 0.0)
    decay_mat = jnp.where(causal, jnp.exp(differ), 0.0)
    key_dots = jnp.einsum('sthd,suhd->shtu', key_unit, key_unit, precision=precise)
    write_heads = jnp.transpose(write_gate, (0, 2, 1))
    strict_part = jnp.where(strict, write_heads[:, :, :, None] * decay_mat * key_dots, 0.0)
    identity = jnp.eye(block_len, dtype=jnp.float32)
    squared = jnp.einsum('shtu,shuv->shtv', strict_part, strict_part, precision=precise)
    fourth = jnp.einsum('shtu,shuv->shtv', squared, squared, precision=precise)
    inverse = jnp.einsum('shtu,shuv->shtv', identity - strict_part, identity + squared, precision=precise)
    inverse = jnp.einsum('shtu,shuv->shtv', inverse, identity + fourth, precision=precise)
    growth = jnp.exp(cumulative)
    target = jnp.einsum('shtu,suhv->sthv', inverse, write_gate[..., None] * value, precision=precise)
    key_mix = jnp.einsum('shtu,suhk->sthk', inverse, (write_gate * growth)[..., None] * key_unit, precision=precise)
    update = target - jnp.einsum('sthk,shkv->sthv', key_mix, state, precision=precise)
    scores = jnp.einsum('sthd,suhd->shtu', query_unit, key_unit, precision=precise) * decay_mat
    attend = jnp.einsum('sthk,shkv->sthv', query_unit * growth[..., None], state, precision=precise)
    attend = attend + jnp.einsum('shtu,suhv->sthv', scores, update, precision=precise)
    final_cum = cumulative[:, -1:, :]
    fading = jnp.exp(final_cum - cumulative)
    new_state = jnp.exp(final_cum[:, 0, :])[:, :, None, None] * state
    new_state = new_state + jnp.einsum('sthk,sthv->shkv', key_unit * fading[..., None], update, precision=precise)
    normed = attend * lax.rsqrt(lax.optimization_barrier(jnp.mean(attend * attend, axis=-1, keepdims=True)) + EPSILON)
    normed = normed * jax.nn.silu(gating) * live[:, :, None, None]
    mixed_heads = normed.reshape(seq_count * block_len, head_count * head_size).astype(jnp.bfloat16)
    return (mixed_heads, new_state)

def reference(tokens, lengths, state, gain_first, first_gate, first_up, first_down, gain_mix, query_weight, key_weight, value_weight, gating_weight, write_weight, forget_weight, forget_rate, out_weight, gain_second, second_gate, second_up, second_down):
    after_first = feed_forward(tokens, gain_first, first_gate, first_up, first_down)
    values = after_first.astype(jnp.float32)
    mix_scale = lax.rsqrt(lax.optimization_barrier(jnp.mean(values * values, axis=1, keepdims=True)) + EPSILON)
    mix_in = (values * gain_mix).astype(jnp.bfloat16)

    def project(matrix):
        return jnp.dot(mix_in, matrix, preferred_element_type=jnp.float32) * mix_scale
    query = project(query_weight).reshape(SEQS, BLK, HEADS, HEAD)
    key_in = project(key_weight).reshape(SEQS, BLK, HEADS, HEAD)
    value = project(value_weight).reshape(SEQS, BLK, HEADS, HEAD)
    gating = project(gating_weight).reshape(SEQS, BLK, HEADS, HEAD)
    write_pre = project(write_weight).reshape(SEQS, BLK, HEADS)
    forget_pre = project(forget_weight).reshape(SEQS, BLK, HEADS)
    positions = jnp.arange(BLK, dtype=jnp.int32)
    live = (positions[None, :] < lengths[:, None]).astype(jnp.float32)
    mixed_heads, new_state = delta_block(query, key_in, value, gating, write_pre, forget_pre, forget_rate, live, state)
    half_cols = HEADS * HEAD // 2
    running = values
    for half_index in range(2):
        portion = jnp.dot(mixed_heads[:, half_index * half_cols:(half_index + 1) * half_cols], out_weight[half_index * half_cols:(half_index + 1) * half_cols], preferred_element_type=jnp.float32)
        rounded = lax.optimization_barrier(portion.astype(jnp.bfloat16)).astype(jnp.float32)
        running = running + rounded
    after_mix = running.astype(jnp.bfloat16)
    mixed_out = feed_forward(after_mix, gain_second, second_gate, second_up, second_down)
    return (mixed_out, new_state)
```

```python
import functools
import math

import jax
import jax.numpy as jnp
from jax import lax
from jax.experimental import pallas as pl
from jax.experimental.pallas import tpu as pltpu
from jax.sharding import PartitionSpec as P

HEADS = 16
HEAD = 128
BLK = 8


EPSILON = 1e-06


def fold_step(gain, gate_cols, up_cols, portion):
    values = portion.astype(jnp.float32)
    scaled = (values * gain).astype(jnp.bfloat16)
    gate_acc = jnp.dot(scaled, gate_cols, preferred_element_type=jnp.float32)
    up_acc = jnp.dot(scaled, up_cols, preferred_element_type=jnp.float32)
    squares = jnp.sum(values * values, axis=1)
    return (gate_acc, up_acc, squares)


def finish_units(gate_acc, up_acc, squares, channels, down_rows):
    row_scale = lax.rsqrt(squares / channels + EPSILON)[:, None]
    hidden = (jax.nn.silu(gate_acc * row_scale) * (up_acc * row_scale)).astype(jnp.bfloat16)
    return jnp.dot(hidden, down_rows, preferred_element_type=jnp.float32)


def feed_forward(hidden_in, gain, w_gate, w_up, w_down):
    channels = gain.shape[0]
    paired = lax.all_to_all(hidden_in, "tp", split_axis=0, concat_axis=1, tiled=True)
    gate_acc, up_acc, squares = fold_step(
        gain, w_gate, w_up, lax.all_gather(paired, "kv", axis=1, tiled=True)
    )
    ffn_term = finish_units(gate_acc, up_acc, squares, channels, w_down)
    partial_value = lax.psum_scatter(ffn_term, "kv", scatter_dimension=1, tiled=True)
    summed = lax.all_to_all(partial_value, "tp", split_axis=1, concat_axis=0, tiled=True)
    return (hidden_in.astype(jnp.float32) + 0.5 * summed).astype(jnp.bfloat16)


def delta_block(query, key_in, value, gating, write_pre, forget_pre, rates, live, state):
    seq_count, block_len, head_count, head_size = query.shape
    precise = lax.Precision.HIGHEST
    query_unit = (
        query
        * lax.rsqrt(jnp.sum(query * query, axis=-1, keepdims=True) + EPSILON)
        / math.sqrt(head_size)
    )
    key_unit = key_in * lax.rsqrt(jnp.sum(key_in * key_in, axis=-1, keepdims=True) + EPSILON)
    live_rows = live[:, :, None]
    write_gate = jax.nn.sigmoid(write_pre) * live_rows
    forget = -jnp.exp(rates)[None, None, :] * jax.nn.softplus(forget_pre) * live_rows
    cumulative = jnp.cumsum(forget, axis=1)
    cum_heads = jnp.transpose(cumulative, (0, 2, 1))
    positions = jnp.arange(block_len)
    causal = positions[:, None] >= positions[None, :]
    strict = positions[:, None] > positions[None, :]
    differ = jnp.minimum(cum_heads[:, :, :, None] - cum_heads[:, :, None, :], 0.0)
    decay_mat = jnp.where(causal, jnp.exp(differ), 0.0)
    key_dots = jnp.einsum("sthd,suhd->shtu", key_unit, key_unit, precision=precise)
    write_heads = jnp.transpose(write_gate, (0, 2, 1))
    strict_part = jnp.where(strict, write_heads[:, :, :, None] * decay_mat * key_dots, 0.0)
    identity = jnp.eye(block_len, dtype=jnp.float32)
    squared = jnp.einsum("shtu,shuv->shtv", strict_part, strict_part, precision=precise)
    fourth = jnp.einsum("shtu,shuv->shtv", squared, squared, precision=precise)
    inverse = jnp.einsum(
        "shtu,shuv->shtv", identity - strict_part, identity + squared, precision=precise
    )
    inverse = jnp.einsum("shtu,shuv->shtv", inverse, identity + fourth, precision=precise)
    growth = jnp.exp(cumulative)
    target = jnp.einsum(
        "shtu,suhv->sthv", inverse, write_gate[..., None] * value, precision=precise
    )
    key_mix = jnp.einsum(
        "shtu,suhk->sthk", inverse, (write_gate * growth)[..., None] * key_unit, precision=precise
    )
    update = target - jnp.einsum("sthk,shkv->sthv", key_mix, state, precision=precise)
    scores = jnp.einsum("sthd,suhd->shtu", query_unit, key_unit, precision=precise) * decay_mat
    attend = jnp.einsum("sthk,shkv->sthv", query_unit * growth[..., None], state, precision=precise)
    attend = attend + jnp.einsum("shtu,suhv->sthv", scores, update, precision=precise)
    final_cum = cumulative[:, -1:, :]
    fading = jnp.exp(final_cum - cumulative)
    new_state = jnp.exp(final_cum[:, 0, :])[:, :, None, None] * state
    new_state = new_state + jnp.einsum(
        "sthk,sthv->shkv", key_unit * fading[..., None], update, precision=precise
    )
    normed = attend * lax.rsqrt(jnp.mean(attend * attend, axis=-1, keepdims=True) + EPSILON)
    normed = normed * jax.nn.silu(gating) * live[:, :, None, None]
    mixed_heads = normed.reshape(seq_count * block_len, head_count * head_size).astype(jnp.bfloat16)
    return (mixed_heads, new_state)


def per_device(
    tokens,
    lengths,
    state,
    gain_first,
    first_gate,
    first_up,
    first_down,
    gain_mix,
    query_weight,
    key_weight,
    value_weight,
    gating_weight,
    write_weight,
    forget_weight,
    forget_rate,
    out_weight,
    gain_second,
    second_gate,
    second_up,
    second_down,
):
    after_first = feed_forward(tokens, gain_first, first_gate, first_up, first_down)
    seq_count = lengths.shape[0]
    own_count = seq_count * BLK
    whole_rows = lax.all_gather(after_first, ("kv", "tp"), axis=1, tiled=True)
    scaled_all = (whole_rows.astype(jnp.float32) * gain_mix).astype(jnp.bfloat16)
    stacked = jnp.stack(
        [
            jnp.dot(scaled_all, matrix, preferred_element_type=jnp.float32)
            for matrix in (query_weight, key_weight, value_weight, gating_weight)
        ]
    )
    owned = lax.all_to_all(
        stacked.astype(jnp.bfloat16), ("kv", "tp"), split_axis=1, concat_axis=2, tiled=True
    ).astype(stacked.dtype)
    row_start = lax.axis_index(("kv", "tp")) * own_count
    own_values = lax.dynamic_slice_in_dim(whole_rows, row_start, own_count, 0).astype(jnp.float32)
    own_scaled = lax.dynamic_slice_in_dim(scaled_all, row_start, own_count, 0)
    mix_scale = lax.rsqrt(jnp.mean(own_values * own_values, axis=1, keepdims=True) + EPSILON)
    query = (owned[0] * mix_scale).reshape(seq_count, BLK, HEADS, HEAD)
    key_in = (owned[1] * mix_scale).reshape(seq_count, BLK, HEADS, HEAD)
    value = (owned[2] * mix_scale).reshape(seq_count, BLK, HEADS, HEAD)
    gating = (owned[3] * mix_scale).reshape(seq_count, BLK, HEADS, HEAD)
    write_pre = (
        jnp.dot(own_scaled, write_weight, preferred_element_type=jnp.float32) * mix_scale
    ).reshape(seq_count, BLK, HEADS)
    forget_pre = (
        jnp.dot(own_scaled, forget_weight, preferred_element_type=jnp.float32) * mix_scale
    ).reshape(seq_count, BLK, HEADS)
    positions = jnp.arange(BLK, dtype=jnp.int32)
    live = (positions[None, :] < lengths[:, None]).astype(jnp.float32)
    mixed_heads, new_state = delta_block(
        query, key_in, value, gating, write_pre, forget_pre, forget_rate, live, state
    )
    half_cols = mixed_heads.shape[1] // 2
    portion = lax.all_gather(mixed_heads, ("kv", "tp"), axis=0, tiled=True)
    first_half = jnp.dot(
        portion[:, :half_cols], out_weight[:half_cols], preferred_element_type=jnp.float32
    ).astype(jnp.bfloat16)
    second_half = jnp.dot(
        portion[:, half_cols:], out_weight[half_cols:], preferred_element_type=jnp.float32
    ).astype(jnp.bfloat16)
    first_half, second_half = lax.optimization_barrier((first_half, second_half))
    mixed_sum = first_half.astype(jnp.float32) + second_half.astype(jnp.float32)
    after_mix = (after_first.astype(jnp.float32) + mixed_sum).astype(jnp.bfloat16)
    mixed_out = feed_forward(after_mix, gain_second, second_gate, second_up, second_down)
    return (mixed_out, new_state)


F32 = jnp.float32
BF16 = jnp.bfloat16
HIGH = lax.Precision.HIGHEST
MESH = pl.DeviceIdType.MESH
VMEM_LIMIT = 60 * 1024 * 1024


def fused_kernel(
    kv_size,
    channels,
    tokens_ref,
    lengths_ref,
    gains1_ref,
    gains_mix_ref,
    gains2_ref,
    rates_ref,
    state_hbm,
    gate1_hbm,
    up1_hbm,
    down1_hbm,
    query_hbm,
    key_hbm,
    value_hbm,
    gating_hbm,
    write_hbm,
    forget_hbm,
    out_hbm,
    gate2_hbm,
    up2_hbm,
    down2_hbm,
    mixed_out_ref,
    new_state_hbm,
    gate1,
    up1,
    down1,
    gate2,
    up2,
    down2,
    proj,
    out_w,
    write_w,
    forget_w,
    state,
    state_out,
    scaled,
    wide,
    narrow,
    gathers,
    heads_all,
    pair_send,
    pair_recv,
    red_send,
    red_recv,
    part_send,
    part_recv,
    load_sems,
    gather_send_sems,
    gather_recv_sems,
    pair_send_sems,
    pair_recv_sems,
    red_send_sems,
    red_recv_sems,
    part_send_sems,
    part_recv_sems,
    store_sem,
):
    kv = lax.axis_index("kv")
    tp = lax.axis_index("tp")
    devices = 2 * kv_size
    me = kv * 2 + tp
    rows, cols = tokens_ref.shape
    take = gate1.shape[1]
    hidden_local = gate1_hbm.shape[1]
    lead = hidden_local - take
    overlap = 2 * take - hidden_local
    first_col = pl.multiple_of(tp * lead, 128)

    def load(index, src, dst):
        return pltpu.make_async_copy(src, dst, load_sems.at[index])

    cut = pl.ds(first_col, take)
    loads = {
        "gate1": load(0, gate1_hbm.at[:, cut], gate1),
        "up1": load(1, up1_hbm.at[:, cut], up1),
        "down1": load(2, down1_hbm.at[cut, :], down1),
        "query": load(3, query_hbm, proj.at[0]),
        "key": load(4, key_hbm, proj.at[1]),
        "value": load(5, value_hbm, proj.at[2]),
        "gating": load(6, gating_hbm, proj.at[3]),
        "write": load(7, write_hbm, write_w),
        "forget": load(8, forget_hbm, forget_w),
        "state": load(9, state_hbm.at[0], state),
        "out": load(10, out_hbm, out_w),
        "gate2": load(11, gate2_hbm.at[:, cut], gate2),
        "up2": load(12, up2_hbm.at[:, cut], up2),
        "down2": load(13, down2_hbm.at[cut, :], down2),
    }
    for name in ("gate1", "up1", "down1"):
        loads[name].start()

    def remote(src, dst, send_sem, recv_sem, to_kv, to_tp):
        return pltpu.make_async_remote_copy(
            src_ref=src,
            dst_ref=dst,
            send_sem=send_sem,
            recv_sem=recv_sem,
            device_id={"kv": to_kv, "tp": to_tp},
            device_id_type=MESH,
        )

    barrier = pltpu.get_barrier_semaphore()
    for off in range(1, devices):
        peer = lax.rem(me + off, devices)
        pl.semaphore_signal(
            barrier,
            inc=1,
            device_id={"kv": peer // 2, "tp": lax.rem(peer, 2)},
            device_id_type=MESH,
        )
    pl.semaphore_wait(barrier, devices - 1)

    def gather_start(phase, buf):
        copies = []
        for off in range(kv_size - 1, 0, -1):
            copies.append(
                remote(
                    buf.at[me],
                    buf.at[me],
                    gather_send_sems.at[phase, off],
                    gather_recv_sems.at[phase, off],
                    lax.rem(kv + off, kv_size),
                    tp,
                )
            )
        copies.append(
            remote(
                buf.at[me],
                buf.at[me],
                gather_send_sems.at[phase, 0],
                gather_recv_sems.at[phase, 0],
                kv,
                1 - tp,
            )
        )
        for copy in copies:
            copy.start()
        return copies

    def gather_finish(phase, buf, copies):
        forwards = []
        for off in range(1, kv_size):
            copies[kv_size - 1 - off].wait_recv()
            slot = lax.rem(kv + kv_size - off, kv_size) * 2 + tp
            forward = remote(
                buf.at[slot],
                buf.at[slot],
                gather_send_sems.at[phase, kv_size - 1 + off],
                gather_recv_sems.at[phase, kv_size - 1 + off],
                kv,
                1 - tp,
            )
            forward.start()
            forwards.append(forward)
        copies[-1].wait_recv()
        for forward in forwards:
            forward.wait_recv()
        for copy in copies + forwards:
            copy.wait_send()

    def scale_rows(buf, gain_ref):
        squares = jnp.zeros((rows, 1), F32)
        for j in range(devices):
            values = buf[j].astype(F32)
            squares = squares + jnp.sum(values * values, axis=1, keepdims=True)
            gain = gain_ref[:, j * cols : (j + 1) * cols]
            scaled[:, j * cols : (j + 1) * cols] = (values * gain).astype(BF16)
        return lax.rsqrt(squares / channels + EPSILON)

    def half_step(phase, buf, gain_ref, names, gate_w, up_w, down_w):
        row_scale = scale_rows(buf, gain_ref)
        loads[names[0]].wait()
        gate = jnp.dot(scaled[...], gate_w[...], preferred_element_type=F32) * row_scale
        loads[names[1]].wait()
        up = jnp.dot(scaled[...], up_w[...], preferred_element_type=F32) * row_scale
        column = lax.broadcasted_iota(jnp.int32, (rows, take), 1)
        hidden = jnp.where(column >= tp * overlap, jax.nn.silu(gate) * up, 0.0).astype(BF16)
        loads[names[2]].wait()

        def columns_of(chip, core):
            at = pl.multiple_of((chip * 2 + core) * cols, cols)
            return jnp.dot(hidden, down_w[:, pl.ds(at, cols)], preferred_element_type=F32)

        order = list(range(kv_size - 1, -1, -1))
        pair_copies = []
        for off in order:
            pair_send[phase, off] = columns_of(lax.rem(kv + off, kv_size), 1 - tp)
            copy = remote(
                pair_send.at[phase, off],
                pair_recv.at[phase, off],
                pair_send_sems.at[phase, off],
                pair_recv_sems.at[phase, off],
                kv,
                1 - tp,
            )
            copy.start()
            pair_copies.append(copy)
        red_copies = []
        total = None
        for position, off in enumerate(order):
            term = columns_of(lax.rem(kv + off, kv_size), tp)
            pair_copies[position].wait_recv()
            term = term + pair_recv[phase, off]
            if off == 0:
                total = term
                continue
            red_send[phase, off] = term.astype(BF16)
            copy = remote(
                red_send.at[phase, off],
                red_recv.at[phase, off],
                red_send_sems.at[phase, off],
                red_recv_sems.at[phase, off],
                lax.rem(kv + off, kv_size),
                tp,
            )
            copy.start()
            red_copies.append(copy)
        for copy in red_copies[::-1]:
            copy.wait_recv()
        for off in range(1, kv_size):
            total = total + red_recv[phase, off].astype(F32)
        for copy in pair_copies + red_copies:
            copy.wait_send()
        return total

    gathers[0, me] = tokens_ref[...]
    copies = gather_start(0, gathers.at[0])
    for name in ("query", "key", "value", "gating", "write", "forget", "state", "out"):
        loads[name].start()
    gather_finish(0, gathers.at[0], copies)
    for name in ("gate2", "up2", "down2"):
        loads[name].start()
    total = half_step(0, gathers.at[0], gains1_ref, ("gate1", "up1", "down1"), gate1, up1, down1)
    after_first = (tokens_ref[...].astype(F32) + 0.5 * total).astype(BF16)
    gathers[1, me] = after_first
    copies = gather_start(1, gathers.at[1])
    gather_finish(1, gathers.at[1], copies)

    mix_scale = scale_rows(gathers.at[1], gains_mix_ref)
    for index, name in enumerate(("query", "key", "value", "gating")):
        loads[name].wait()
        product = jnp.dot(scaled[...], proj[index], preferred_element_type=F32) * mix_scale
        part_send[:, :, index * cols : (index + 1) * cols] = product.reshape(
            devices, BLK, cols
        ).astype(BF16)
    part_copies = []
    for off in range(1, devices):
        peer = lax.rem(me + off, devices)
        copy = remote(
            part_send.at[peer],
            part_recv.at[me],
            part_send_sems.at[off],
            part_recv_sems.at[off],
            peer // 2,
            lax.rem(peer, 2),
        )
        copy.start()
        part_copies.append(copy)
    part_recv[me] = part_send[me]
    loads["write"].wait()
    loads["forget"].wait()
    wide[:, 0:HEADS] = jnp.dot(scaled[...], write_w[...], preferred_element_type=F32) * mix_scale
    narrow[:, 0:HEADS] = jnp.dot(scaled[...], forget_w[...], preferred_element_type=F32) * mix_scale
    own = pl.ds(pl.multiple_of(me * BLK, BLK), BLK)
    write_pre = wide[own, 0:HEADS]
    forget_pre = narrow[own, 0:HEADS]

    size = HEADS * BLK
    row = lax.broadcasted_iota(jnp.int32, (size, size), 0)
    col = lax.broadcasted_iota(jnp.int32, (size, size), 1)
    same = (row // BLK) == (col // BLK)
    causal = same & (row >= col)
    strict = same & (row > col)
    diagonal = row == col
    identity = jnp.where(diagonal, 1.0, 0.0)
    head_row = lax.broadcasted_iota(jnp.int32, (size, HEADS), 0) // BLK
    head_col = lax.broadcasted_iota(jnp.int32, (size, HEADS), 1)
    pick = head_row == head_col

    def as_column(block):
        return jnp.sum(jnp.where(pick, block, 0.0), axis=1, keepdims=True)

    def to_row(column):
        return jnp.sum(jnp.where(diagonal, column, 0.0), axis=0, keepdims=True)

    token_at = lax.rem(lax.broadcasted_iota(jnp.int32, (size, 1), 0), BLK)
    live = jnp.where(token_at < lengths_ref[0], 1.0, 0.0)
    write_col = as_column(jnp.concatenate([write_pre] * HEADS, axis=0))
    forget_col = as_column(jnp.concatenate([forget_pre] * HEADS, axis=0))
    rate_col = as_column(jnp.broadcast_to(rates_ref[...], (size, HEADS)))
    write_gate = jax.nn.sigmoid(write_col) * live
    softplus = jnp.maximum(forget_col, 0.0) + jnp.log1p(jnp.exp(-jnp.abs(forget_col)))
    forget = -jnp.exp(rate_col) * softplus * live
    forget_row = to_row(forget)
    cumulative = jnp.sum(jnp.where(causal, forget_row, 0.0), axis=1, keepdims=True)
    final = jnp.sum(jnp.where(same, forget_row, 0.0), axis=1, keepdims=True)
    decay = jnp.where(causal, jnp.exp(jnp.minimum(cumulative - to_row(cumulative), 0.0)), 0.0)
    growth = jnp.exp(cumulative)
    fading = jnp.exp(final - cumulative)
    shrink = jnp.exp(final)

    for copy in part_copies:
        copy.wait_recv()

    def by_head(index):
        pieces = []
        for j in range(devices):
            block = part_recv[j, :, index * cols : (index + 1) * cols].astype(F32)
            for at in range(0, cols, HEAD):
                pieces.append(block[:, at : at + HEAD])
        return jnp.concatenate(pieces, axis=0)

    def dot(a, b, dims=((1,), (0,))):
        return lax.dot_general(a, b, (dims, ((), ())), precision=HIGH, preferred_element_type=F32)

    query, key_in, value, gating = (by_head(index) for index in range(4))
    query_unit = (
        query
        * lax.rsqrt(jnp.sum(query * query, axis=1, keepdims=True) + EPSILON)
        * (1.0 / math.sqrt(HEAD))
    )
    key_unit = key_in * lax.rsqrt(jnp.sum(key_in * key_in, axis=1, keepdims=True) + EPSILON)
    lower = dot(key_unit, key_unit, ((1,), (1,)))
    lower = jnp.where(strict, write_gate * decay * lower, 0.0)
    squared = dot(lower, lower)
    fourth = dot(squared, squared)
    inverse = dot(identity - lower, identity + squared)
    inverse = dot(inverse, identity + fourth)
    target = dot(inverse, write_gate * value)
    key_mix = dot(inverse, (write_gate * growth) * key_unit)
    query_grown = query_unit * growth
    scores = dot(query_unit, key_unit, ((1,), (1,))) * decay
    loads["state"].wait()
    key_terms, query_terms = [], []
    for head in range(HEADS):
        at = slice(head * BLK, (head + 1) * BLK)
        both = jnp.concatenate([key_mix[at], query_grown[at]], axis=0)
        result = dot(both, state[head])
        key_terms.append(result[:BLK])
        query_terms.append(result[BLK:])
    update = target - jnp.concatenate(key_terms, axis=0)
    attend = jnp.concatenate(query_terms, axis=0) + dot(scores, update)
    normed = attend * lax.rsqrt(jnp.mean(attend * attend, axis=1, keepdims=True) + EPSILON)
    normed = normed * jax.nn.silu(gating) * live
    heads_all[me] = jnp.concatenate(
        [normed[head * BLK : (head + 1) * BLK] for head in range(HEADS)], axis=1
    ).astype(BF16)
    copies = gather_start(2, heads_all)
    faded = key_unit * fading
    for head in range(HEADS):
        at = slice(head * BLK, (head + 1) * BLK)
        outer = dot(faded[at], update[at], ((0,), (0,)))
        state_out[head] = shrink[head * BLK : head * BLK + 1] * state[head] + outer
    store = pltpu.make_async_copy(state_out, new_state_hbm.at[0], store_sem)
    store.start()
    gather_finish(2, heads_all, copies)

    mixed = heads_all[...].astype(F32).reshape(rows, HEADS * HEAD).astype(BF16)
    loads["out"].wait()
    half = HEADS * HEAD // 2
    first = jnp.dot(mixed[:, :half], out_w[:half], preferred_element_type=F32).astype(BF16)
    second = jnp.dot(mixed[:, half:], out_w[half:], preferred_element_type=F32).astype(BF16)
    residual = gathers[1, me].astype(F32)
    after_mix = (residual + (first.astype(F32) + second.astype(F32))).astype(BF16)
    gathers[2, me] = after_mix
    copies = gather_start(3, gathers.at[2])
    gather_finish(3, gathers.at[2], copies)

    total = half_step(1, gathers.at[2], gains2_ref, ("gate2", "up2", "down2"), gate2, up2, down2)
    mixed_out_ref[...] = (gathers[2, me].astype(F32) + 0.5 * total).astype(BF16)
    for copy in part_copies:
        copy.wait_send()
    store.wait()


def fused_call(mesh, *args):
    (
        tokens, lengths, state, gain_first, first_gate, first_up, first_down, gain_mix,
        query_weight, key_weight, value_weight, gating_weight, write_weight, forget_weight,
        forget_rate, out_weight, gain_second, second_gate, second_up, second_down,
    ) = args
    kv_size = mesh.shape["kv"]
    devices = kv_size * mesh.shape["tp"]
    rows, cols = tokens.shape
    channels = gain_first.shape[0]
    hidden_local = first_gate.shape[1]
    take = -(-hidden_local // 256) * 128
    phases = 2
    in_vmem = pl.BlockSpec(memory_space=pltpu.VMEM)
    in_smem = pl.BlockSpec(memory_space=pltpu.SMEM)
    in_any = pl.BlockSpec(memory_space=pl.ANY)
    dma = pltpu.SemaphoreType.DMA
    return pl.pallas_call(
        functools.partial(fused_kernel, kv_size, channels),
        out_shape=(
            jax.ShapeDtypeStruct(tokens.shape, tokens.dtype),
            jax.ShapeDtypeStruct(state.shape, state.dtype),
        ),
        in_specs=[in_vmem, in_smem] + [in_vmem] * 4 + [in_any] * 14,
        out_specs=(in_vmem, in_any),
        scratch_shapes=[
            pltpu.VMEM((channels, take), BF16),
            pltpu.VMEM((channels, take), BF16),
            pltpu.VMEM((take, channels), BF16),
            pltpu.VMEM((channels, take), BF16),
            pltpu.VMEM((channels, take), BF16),
            pltpu.VMEM((take, channels), BF16),
            pltpu.VMEM((4,) + query_weight.shape, BF16),
            pltpu.VMEM(out_weight.shape, BF16),
            pltpu.VMEM(write_weight.shape, BF16),
            pltpu.VMEM(forget_weight.shape, BF16),
            pltpu.VMEM(state.shape[1:], F32),
            pltpu.VMEM(state.shape[1:], F32),
            pltpu.VMEM((rows, channels), BF16),
            pltpu.VMEM((rows, 128), F32),
            pltpu.VMEM((rows, 128), F32),
            pltpu.VMEM((3, devices, rows, cols), BF16),
            pltpu.VMEM((devices, BLK, HEADS * HEAD), BF16),
            pltpu.VMEM((phases, kv_size, rows, cols), F32),
            pltpu.VMEM((phases, kv_size, rows, cols), F32),
            pltpu.VMEM((phases, kv_size, rows, cols), BF16),
            pltpu.VMEM((phases, kv_size, rows, cols), BF16),
            pltpu.VMEM((devices, BLK, 4 * cols), BF16),
            pltpu.VMEM((devices, BLK, 4 * cols), BF16),
            dma((14,)),
            dma((4, 2 * kv_size)),
            dma((4, 2 * kv_size)),
            dma((phases, kv_size)),
            dma((phases, kv_size)),
            dma((phases, kv_size)),
            dma((phases, kv_size)),
            dma((devices,)),
            dma((devices,)),
            dma,
        ],
        compiler_params=pltpu.CompilerParams(
            collective_id=0, has_side_effects=True, vmem_limit_bytes=VMEM_LIMIT
        ),
    )(
        tokens, lengths, gain_first.reshape(1, -1), gain_mix.reshape(1, -1),
        gain_second.reshape(1, -1), forget_rate.reshape(1, -1), state,
        first_gate, first_up, first_down, query_weight, key_weight, value_weight,
        gating_weight, write_weight, forget_weight, out_weight, second_gate, second_up,
        second_down,
    )


def fits_fused(mesh, args):
    tokens, lengths, state, first_gate = args[0], args[1], args[2], args[4]
    rows, cols = tokens.shape
    devices = mesh.shape["kv"] * mesh.shape["tp"]
    return (
        mesh.shape["tp"] == 2
        and lengths.shape[0] == 1
        and rows == devices * BLK
        and cols % 256 == 0
        and first_gate.shape[1] % 128 == 0
        and state.shape[1:] == (HEADS, HEAD, HEAD)
    )


def solution(mesh):
    in_specs = (
        P("dp", ("kv", "tp")),
        P(("dp", "kv", "tp")),
        P(("dp", "kv", "tp"), None, None, None),
        P(),
        P(None, "kv"),
        P(None, "kv"),
        P("kv", None),
        P(),
        P(None, ("kv", "tp")),
        P(None, ("kv", "tp")),
        P(None, ("kv", "tp")),
        P(None, ("kv", "tp")),
        P(),
        P(),
        P(),
        P(None, ("kv", "tp")),
        P(),
        P(None, "kv"),
        P(None, "kv"),
        P("kv", None),
    )
    out_specs = (P("dp", ("kv", "tp")), P(("dp", "kv", "tp"), None, None, None))

    def body(*args):
        if fits_fused(mesh, args):
            return fused_call(mesh, *args)
        return per_device(*args)

    return jax.shard_map(
        body, mesh=mesh, in_specs=in_specs, out_specs=out_specs, check_vma=False
    )
```

```python
import functools
import math

import jax
import jax.numpy as jnp
from jax import lax
from jax.experimental import pallas as pl
from jax.experimental.pallas import tpu as pltpu
from jax.sharding import PartitionSpec as P

HEADS = 16
HEAD = 128
BLK = 8


EPSILON = 1e-06


def fold_step(gain, gate_cols, up_cols, portion):
    values = portion.astype(jnp.float32)
    scaled = (values * gain).astype(jnp.bfloat16)
    gate_acc = jnp.dot(scaled, gate_cols, preferred_element_type=jnp.float32)
    up_acc = jnp.dot(scaled, up_cols, preferred_element_type=jnp.float32)
    squares = jnp.sum(values * values, axis=1)
    return (gate_acc, up_acc, squares)


def finish_units(gate_acc, up_acc, squares, channels, down_rows):
    row_scale = lax.rsqrt(squares / channels + EPSILON)[:, None]
    hidden = (jax.nn.silu(gate_acc * row_scale) * (up_acc * row_scale)).astype(jnp.bfloat16)
    return jnp.dot(hidden, down_rows, preferred_element_type=jnp.float32)


def feed_forward(hidden_in, gain, w_gate, w_up, w_down):
    channels = gain.shape[0]
    paired = lax.all_to_all(hidden_in, "tp", split_axis=0, concat_axis=1, tiled=True)
    gate_acc, up_acc, squares = fold_step(
        gain, w_gate, w_up, lax.all_gather(paired, "kv", axis=1, tiled=True)
    )
    ffn_term = finish_units(gate_acc, up_acc, squares, channels, w_down)
    partial_value = lax.psum_scatter(ffn_term, "kv", scatter_dimension=1, tiled=True)
    summed = lax.all_to_all(partial_value, "tp", split_axis=1, concat_axis=0, tiled=True)
    return (hidden_in.astype(jnp.float32) + 0.5 * summed).astype(jnp.bfloat16)


def delta_block(query, key_in, value, gating, write_pre, forget_pre, rates, live, state):
    seq_count, block_len, head_count, head_size = query.shape
    precise = lax.Precision.HIGHEST
    query_unit = (
        query
        * lax.rsqrt(jnp.sum(query * query, axis=-1, keepdims=True) + EPSILON)
        / math.sqrt(head_size)
    )
    key_unit = key_in * lax.rsqrt(jnp.sum(key_in * key_in, axis=-1, keepdims=True) + EPSILON)
    live_rows = live[:, :, None]
    write_gate = jax.nn.sigmoid(write_pre) * live_rows
    forget = -jnp.exp(rates)[None, None, :] * jax.nn.softplus(forget_pre) * live_rows
    cumulative = jnp.cumsum(forget, axis=1)
    cum_heads = jnp.transpose(cumulative, (0, 2, 1))
    positions = jnp.arange(block_len)
    causal = positions[:, None] >= positions[None, :]
    strict = positions[:, None] > positions[None, :]
    differ = jnp.minimum(cum_heads[:, :, :, None] - cum_heads[:, :, None, :], 0.0)
    decay_mat = jnp.where(causal, jnp.exp(differ), 0.0)
    key_dots = jnp.einsum("sthd,suhd->shtu", key_unit, key_unit, precision=precise)
    write_heads = jnp.transpose(write_gate, (0, 2, 1))
    strict_part = jnp.where(strict, write_heads[:, :, :, None] * decay_mat * key_dots, 0.0)
    identity = jnp.eye(block_len, dtype=jnp.float32)
    squared = jnp.einsum("shtu,shuv->shtv", strict_part, strict_part, precision=precise)
    fourth = jnp.einsum("shtu,shuv->shtv", squared, squared, precision=precise)
    inverse = jnp.einsum(
        "shtu,shuv->shtv", identity - strict_part, identity + squared, precision=precise
    )
    inverse = jnp.einsum("shtu,shuv->shtv", inverse, identity + fourth, precision=precise)
    growth = jnp.exp(cumulative)
    target = jnp.einsum(
        "shtu,suhv->sthv", inverse, write_gate[..., None] * value, precision=precise
    )
    key_mix = jnp.einsum(
        "shtu,suhk->sthk", inverse, (write_gate * growth)[..., None] * key_unit, precision=precise
    )
    update = target - jnp.einsum("sthk,shkv->sthv", key_mix, state, precision=precise)
    scores = jnp.einsum("sthd,suhd->shtu", query_unit, key_unit, precision=precise) * decay_mat
    attend = jnp.einsum("sthk,shkv->sthv", query_unit * growth[..., None], state, precision=precise)
    attend = attend + jnp.einsum("shtu,suhv->sthv", scores, update, precision=precise)
    final_cum = cumulative[:, -1:, :]
    fading = jnp.exp(final_cum - cumulative)
    new_state = jnp.exp(final_cum[:, 0, :])[:, :, None, None] * state
    new_state = new_state + jnp.einsum(
        "sthk,sthv->shkv", key_unit * fading[..., None], update, precision=precise
    )
    normed = attend * lax.rsqrt(jnp.mean(attend * attend, axis=-1, keepdims=True) + EPSILON)
    normed = normed * jax.nn.silu(gating) * live[:, :, None, None]
    mixed_heads = normed.reshape(seq_count * block_len, head_count * head_size).astype(jnp.bfloat16)
    return (mixed_heads, new_state)


def per_device(
    tokens,
    lengths,
    state,
    gain_first,
    first_gate,
    first_up,
    first_down,
    gain_mix,
    query_weight,
    key_weight,
    value_weight,
    gating_weight,
    write_weight,
    forget_weight,
    forget_rate,
    out_weight,
    gain_second,
    second_gate,
    second_up,
    second_down,
):
    after_first = feed_forward(tokens, gain_first, first_gate, first_up, first_down)
    seq_count = lengths.shape[0]
    own_count = seq_count * BLK
    whole_rows = lax.all_gather(after_first, ("kv", "tp"), axis=1, tiled=True)
    scaled_all = (whole_rows.astype(jnp.float32) * gain_mix).astype(jnp.bfloat16)
    stacked = jnp.stack(
        [
            jnp.dot(scaled_all, matrix, preferred_element_type=jnp.float32)
            for matrix in (query_weight, key_weight, value_weight, gating_weight)
        ]
    )
    owned = lax.all_to_all(
        stacked.astype(jnp.bfloat16), ("kv", "tp"), split_axis=1, concat_axis=2, tiled=True
    ).astype(stacked.dtype)
    row_start = lax.axis_index(("kv", "tp")) * own_count
    own_values = lax.dynamic_slice_in_dim(whole_rows, row_start, own_count, 0).astype(jnp.float32)
    own_scaled = lax.dynamic_slice_in_dim(scaled_all, row_start, own_count, 0)
    mix_scale = lax.rsqrt(jnp.mean(own_values * own_values, axis=1, keepdims=True) + EPSILON)
    query = (owned[0] * mix_scale).reshape(seq_count, BLK, HEADS, HEAD)
    key_in = (owned[1] * mix_scale).reshape(seq_count, BLK, HEADS, HEAD)
    value = (owned[2] * mix_scale).reshape(seq_count, BLK, HEADS, HEAD)
    gating = (owned[3] * mix_scale).reshape(seq_count, BLK, HEADS, HEAD)
    write_pre = (
        jnp.dot(own_scaled, write_weight, preferred_element_type=jnp.float32) * mix_scale
    ).reshape(seq_count, BLK, HEADS)
    forget_pre = (
        jnp.dot(own_scaled, forget_weight, preferred_element_type=jnp.float32) * mix_scale
    ).reshape(seq_count, BLK, HEADS)
    positions = jnp.arange(BLK, dtype=jnp.int32)
    live = (positions[None, :] < lengths[:, None]).astype(jnp.float32)
    mixed_heads, new_state = delta_block(
        query, key_in, value, gating, write_pre, forget_pre, forget_rate, live, state
    )
    half_cols = mixed_heads.shape[1] // 2
    portion = lax.all_gather(mixed_heads, ("kv", "tp"), axis=0, tiled=True)
    first_half = jnp.dot(
        portion[:, :half_cols], out_weight[:half_cols], preferred_element_type=jnp.float32
    ).astype(jnp.bfloat16)
    second_half = jnp.dot(
        portion[:, half_cols:], out_weight[half_cols:], preferred_element_type=jnp.float32
    ).astype(jnp.bfloat16)
    first_half, second_half = lax.optimization_barrier((first_half, second_half))
    mixed_sum = first_half.astype(jnp.float32) + second_half.astype(jnp.float32)
    after_mix = (after_first.astype(jnp.float32) + mixed_sum).astype(jnp.bfloat16)
    mixed_out = feed_forward(after_mix, gain_second, second_gate, second_up, second_down)
    return (mixed_out, new_state)


F32 = jnp.float32
BF16 = jnp.bfloat16
HIGH = lax.Precision.HIGHEST
MESH = pl.DeviceIdType.MESH
VMEM_LIMIT = 60 * 1024 * 1024


def fused_kernel(
    kv_size,
    channels,
    tokens_ref,
    lengths_ref,
    gains1_ref,
    gains_mix_ref,
    gains2_ref,
    rates_ref,
    state_hbm,
    gate1_hbm,
    up1_hbm,
    down1_hbm,
    query_hbm,
    key_hbm,
    value_hbm,
    gating_hbm,
    write_hbm,
    forget_hbm,
    out_hbm,
    gate2_hbm,
    up2_hbm,
    down2_hbm,
    mixed_out_ref,
    new_state_hbm,
    gate1,
    up1,
    down1,
    gate2,
    up2,
    down2,
    proj,
    out_w,
    small_w,
    state,
    state_high,
    state_low,
    state_out,
    gate_acc,
    up_acc,
    proj_acc,
    small_acc,
    gathers,
    heads_all,
    pair_send,
    pair_recv,
    red_send,
    red_recv,
    part_send,
    part_recv,
    load_sems,
    gather_send_sems,
    gather_recv_sems,
    pair_send_sems,
    pair_recv_sems,
    red_send_sems,
    red_recv_sems,
    part_send_sems,
    part_recv_sems,
    store_sem,
):
    kv = lax.axis_index("kv")
    tp = lax.axis_index("tp")
    devices = 2 * kv_size
    me = kv * 2 + tp
    rows, cols = tokens_ref.shape
    take = gate1.shape[1]
    hidden_local = gate1_hbm.shape[1]
    lead = hidden_local - take
    overlap = 2 * take - hidden_local
    first_col = pl.multiple_of(tp * lead, 128)

    def load(index, src, dst):
        return pltpu.make_async_copy(src, dst, load_sems.at[index])

    cut = pl.ds(first_col, take)
    loads = {
        "gate1": load(0, gate1_hbm.at[:, cut], gate1),
        "up1": load(1, up1_hbm.at[:, cut], up1),
        "down1": load(2, down1_hbm.at[cut, :], down1),
        "query": load(3, query_hbm, proj.at[:, 0:cols]),
        "key": load(4, key_hbm, proj.at[:, cols : 2 * cols]),
        "value": load(5, value_hbm, proj.at[:, 2 * cols : 3 * cols]),
        "gating": load(6, gating_hbm, proj.at[:, 3 * cols : 4 * cols]),
        "write": load(7, write_hbm, small_w.at[0:HEADS]),
        "forget": load(8, forget_hbm, small_w.at[HEADS : 2 * HEADS]),
        "state": load(9, state_hbm.at[0], state),
        "out": load(10, out_hbm, out_w),
        "gate2": load(11, gate2_hbm.at[:, cut], gate2),
        "up2": load(12, up2_hbm.at[:, cut], up2),
        "down2": load(13, down2_hbm.at[cut, :], down2),
    }
    for name in ("gate1", "up1", "down1"):
        loads[name].start()

    def remote(src, dst, send_sem, recv_sem, to_kv, to_tp):
        return pltpu.make_async_remote_copy(
            src_ref=src,
            dst_ref=dst,
            send_sem=send_sem,
            recv_sem=recv_sem,
            device_id={"kv": to_kv, "tp": to_tp},
            device_id_type=MESH,
        )

    barrier = pltpu.get_barrier_semaphore()
    for off in range(1, devices):
        peer = lax.rem(me + off, devices)
        pl.semaphore_signal(
            barrier,
            inc=1,
            device_id={"kv": peer // 2, "tp": lax.rem(peer, 2)},
            device_id_type=MESH,
        )
    pl.semaphore_wait(barrier, devices - 1)

    def swapped(off):
        chip, bit = kv, 1
        while bit < kv_size:
            if off & bit:
                chip = chip + bit - 2 * bit * lax.rem(kv // bit, 2)
            bit *= 2
        return chip

    def gather_start(phase, buf):
        copies = {}
        for off in list(range(kv_size - 1, 0, -1)) + [0]:
            copies[off] = remote(
                buf.at[me],
                buf.at[me],
                gather_send_sems.at[phase, off],
                gather_recv_sems.at[phase, off],
                swapped(off),
                1 - tp if off == 0 else tp,
            )
            copies[off].start()
        return copies

    def gather_finish(phase, buf, copies, use=lambda slot, first: None):
        use(me, True)
        copies[0].wait_recv()
        use(kv * 2 + 1 - tp, False)
        forwards = {}
        for off in range(1, kv_size):
            copies[off].wait_recv()
            slot = swapped(off) * 2 + tp
            forwards[off] = remote(
                buf.at[slot],
                buf.at[slot],
                gather_send_sems.at[phase, kv_size - 1 + off],
                gather_recv_sems.at[phase, kv_size - 1 + off],
                kv,
                1 - tp,
            )
            forwards[off].start()
        for off in range(1, kv_size):
            use(swapped(off) * 2 + tp, False)
        for off in range(1, kv_size):
            forwards[off].wait_recv()
            use(swapped(off) * 2 + 1 - tp, False)
        for off in range(kv_size):
            copies[off].wait_send()
        for off in range(1, kv_size):
            forwards[off].wait_send()

    def multiply(buf, gain_ref, products):
        squares = [jnp.zeros((rows, 1), F32)]

        def use(slot, first):
            at = pl.ds(pl.multiple_of(slot * cols, cols), cols)
            values = buf[slot].astype(F32)
            squares[0] = squares[0] + jnp.sum(values * values, axis=1, keepdims=True)
            scaled = (values * gain_ref[:, at]).astype(BF16)
            for acc, weight, across in products:
                if across:
                    term = lax.dot_general(
                        scaled,
                        weight[:, at],
                        (((1,), (1,)), ((), ())),
                        preferred_element_type=F32,
                    )
                else:
                    term = jnp.dot(scaled, weight[at, :], preferred_element_type=F32)
                if first:
                    acc[...] = term
                else:
                    acc[...] += term

        return squares, use

    def inverse_rms(squares):
        return lax.rsqrt(squares[0] / channels + EPSILON)

    def half_step(phase, at, buf, copies, gain_ref, names, gate_w, up_w, down_w):
        loads[names[0]].wait()
        loads[names[1]].wait()
        squares, use = multiply(buf, gain_ref, ((gate_acc, gate_w, False), (up_acc, up_w, False)))
        gather_finish(at, buf, copies, use)
        row_scale = inverse_rms(squares)
        gate = gate_acc[...] * row_scale
        up = up_acc[...] * row_scale
        column = lax.broadcasted_iota(jnp.int32, (rows, take), 1)
        hidden = jnp.where(column >= tp * overlap, jax.nn.silu(gate) * up, 0.0).astype(BF16)
        loads[names[2]].wait()

        def columns_of(chip, core):
            at = pl.multiple_of((chip * 2 + core) * cols, cols)
            return jnp.dot(hidden, down_w[:, pl.ds(at, cols)], preferred_element_type=F32)

        order = list(range(kv_size - 1, -1, -1))
        pair_copies = []
        for off in order:
            pair_send[phase, off] = columns_of(swapped(off), 1 - tp)
            copy = remote(
                pair_send.at[phase, off],
                pair_recv.at[phase, off],
                pair_send_sems.at[phase, off],
                pair_recv_sems.at[phase, off],
                kv,
                1 - tp,
            )
            copy.start()
            pair_copies.append(copy)
        red_copies = []
        total = None
        for position, off in enumerate(order):
            term = columns_of(swapped(off), tp)
            pair_copies[position].wait_recv()
            term = term + pair_recv[phase, off]
            if off == 0:
                total = term
                continue
            red_send[phase, off] = term.astype(BF16)
            copy = remote(
                red_send.at[phase, off],
                red_recv.at[phase, off],
                red_send_sems.at[phase, off],
                red_recv_sems.at[phase, off],
                swapped(off),
                tp,
            )
            copy.start()
            red_copies.append(copy)
        for copy in red_copies[::-1]:
            copy.wait_recv()
        for off in range(1, kv_size):
            total = total + red_recv[phase, off].astype(F32)
        for copy in pair_copies + red_copies:
            copy.wait_send()
        return total

    gathers[0, me] = tokens_ref[...]
    copies = gather_start(0, gathers.at[0])
    for name in ("query", "key", "value", "gating", "write", "forget", "state", "out"):
        loads[name].start()
    for name in ("gate2", "up2", "down2"):
        loads[name].start()
    total = half_step(
        0, 0, gathers.at[0], copies, gains1_ref, ("gate1", "up1", "down1"), gate1, up1, down1
    )
    after_first = (tokens_ref[...].astype(F32) + 0.5 * total).astype(BF16)
    gathers[1, me] = after_first
    copies = gather_start(1, gathers.at[1])

    loads["state"].wait()
    for head in range(HEADS):
        high = state[head].astype(BF16)
        state_high[head] = high
        state_low[head] = (state[head] - high.astype(F32)).astype(BF16)
    for name in ("query", "key", "value", "gating", "write", "forget"):
        loads[name].wait()
    squares, use = multiply(
        gathers.at[1], gains_mix_ref, ((proj_acc, proj, False), (small_acc, small_w, True))
    )
    gather_finish(1, gathers.at[1], copies, use)
    mix_scale = inverse_rms(squares)
    part_send[...] = (proj_acc[...] * mix_scale).reshape(devices, BLK, 4 * cols).astype(BF16)
    part_copies = []
    for off in range(1, devices):
        peer = lax.rem(me + off, devices)
        copy = remote(
            part_send.at[peer],
            part_recv.at[me],
            part_send_sems.at[off],
            part_recv_sems.at[off],
            peer // 2,
            lax.rem(peer, 2),
        )
        copy.start()
        part_copies.append(copy)
    part_recv[me] = part_send[me]
    small_acc[...] = small_acc[...] * mix_scale
    own = pl.ds(pl.multiple_of(me * BLK, BLK), BLK)
    write_pre = small_acc[own, 0:HEADS]
    forget_pre = small_acc[own, HEADS : 2 * HEADS]

    size = HEADS * BLK
    row = lax.broadcasted_iota(jnp.int32, (size, size), 0)
    col = lax.broadcasted_iota(jnp.int32, (size, size), 1)
    same = (row // BLK) == (col // BLK)
    causal = same & (row >= col)
    strict = same & (row > col)
    diagonal = row == col
    identity = jnp.where(diagonal, 1.0, 0.0)
    head_row = lax.broadcasted_iota(jnp.int32, (size, HEADS), 0) // BLK
    head_col = lax.broadcasted_iota(jnp.int32, (size, HEADS), 1)
    pick = head_row == head_col

    def as_column(block):
        return jnp.sum(jnp.where(pick, block, 0.0), axis=1, keepdims=True)

    def to_row(column):
        return jnp.sum(jnp.where(diagonal, column, 0.0), axis=0, keepdims=True)

    token_at = lax.rem(lax.broadcasted_iota(jnp.int32, (size, 1), 0), BLK)
    live = jnp.where(token_at < lengths_ref[0], 1.0, 0.0)
    write_col = as_column(jnp.concatenate([write_pre] * HEADS, axis=0))
    forget_col = as_column(jnp.concatenate([forget_pre] * HEADS, axis=0))
    rate_col = as_column(jnp.broadcast_to(rates_ref[...], (size, HEADS)))
    write_gate = jax.nn.sigmoid(write_col) * live
    softplus = jnp.maximum(forget_col, 0.0) + jnp.log1p(jnp.exp(-jnp.abs(forget_col)))
    forget = -jnp.exp(rate_col) * softplus * live
    forget_row = to_row(forget)
    cumulative = jnp.sum(jnp.where(causal, forget_row, 0.0), axis=1, keepdims=True)
    final = jnp.sum(jnp.where(same, forget_row, 0.0), axis=1, keepdims=True)
    decay = jnp.where(causal, jnp.exp(jnp.minimum(cumulative - to_row(cumulative), 0.0)), 0.0)
    growth = jnp.exp(cumulative)
    fading = jnp.exp(final - cumulative)
    shrink = jnp.exp(final)

    for copy in part_copies:
        copy.wait_recv()

    def by_head(index):
        pieces = []
        for j in range(devices):
            block = part_recv[j, :, index * cols : (index + 1) * cols].astype(F32)
            for at in range(0, cols, HEAD):
                pieces.append(block[:, at : at + HEAD])
        return jnp.concatenate(pieces, axis=0)

    def dot(a, b, dims=((1,), (0,))):
        return lax.dot_general(a, b, (dims, ((), ())), precision=HIGH, preferred_element_type=F32)

    query, key_in, value, gating = (by_head(index) for index in range(4))
    query_unit = (
        query
        * lax.rsqrt(jnp.sum(query * query, axis=1, keepdims=True) + EPSILON)
        * (1.0 / math.sqrt(HEAD))
    )
    key_unit = key_in * lax.rsqrt(jnp.sum(key_in * key_in, axis=1, keepdims=True) + EPSILON)
    lower = dot(key_unit, key_unit, ((1,), (1,)))
    lower = jnp.where(strict, write_gate * decay * lower, 0.0)
    squared = dot(lower, lower)
    fourth = dot(squared, squared)
    inverse = dot(identity - lower, identity + squared)
    inverse = dot(inverse, identity + fourth)
    key_grown = (write_gate * growth) * key_unit
    query_grown = query_unit * growth
    scores = dot(query_unit, key_unit, ((1,), (1,))) * decay

    def cut_terms(a):
        high = a.astype(BF16).astype(F32)
        return high, a - high

    key_terms, query_terms = [], []
    for head in range(HEADS):
        at = slice(head * BLK, (head + 1) * BLK)
        high, low = cut_terms(jnp.concatenate([key_grown[at], query_grown[at]], axis=0))
        both = jnp.concatenate([high, low], axis=0).astype(BF16)
        result = jnp.dot(both, state_high[head], preferred_element_type=F32)
        result = result[: 2 * BLK] + result[2 * BLK :]
        result = result + jnp.dot(
            both[: 2 * BLK], state_low[head], preferred_element_type=F32
        )
        key_terms.append(result[:BLK])
        query_terms.append(result[BLK:])
    update = dot(inverse, write_gate * value - jnp.concatenate(key_terms, axis=0))
    attend = jnp.concatenate(query_terms, axis=0) + dot(scores, update)
    normed = attend * lax.rsqrt(jnp.mean(attend * attend, axis=1, keepdims=True) + EPSILON)
    normed = normed * jax.nn.silu(gating) * live
    heads_all[me] = jnp.concatenate(
        [normed[head * BLK : (head + 1) * BLK] for head in range(HEADS)], axis=1
    ).astype(BF16)
    copies = gather_start(2, heads_all)
    faded = key_unit * fading
    for head in range(HEADS):
        at = slice(head * BLK, (head + 1) * BLK)
        key_high, key_low = cut_terms(faded[at])
        value_high, value_low = cut_terms(update[at])
        outer = lax.dot_general(
            jnp.concatenate([key_high, key_high, key_low], axis=0).astype(BF16),
            jnp.concatenate([value_high, value_low, value_high], axis=0).astype(BF16),
            (((0,), (0,)), ((), ())),
            preferred_element_type=F32,
        )
        state_out[head] = shrink[head * BLK : head * BLK + 1] * state[head] + outer
    store = pltpu.make_async_copy(state_out, new_state_hbm.at[0], store_sem)
    store.start()
    gather_finish(2, heads_all, copies)

    mixed = heads_all[...].astype(F32).reshape(rows, HEADS * HEAD).astype(BF16)
    loads["out"].wait()
    half = HEADS * HEAD // 2
    first = jnp.dot(mixed[:, :half], out_w[:half], preferred_element_type=F32).astype(BF16)
    second = jnp.dot(mixed[:, half:], out_w[half:], preferred_element_type=F32).astype(BF16)
    residual = gathers[1, me].astype(F32)
    after_mix = (residual + (first.astype(F32) + second.astype(F32))).astype(BF16)
    gathers[2, me] = after_mix
    copies = gather_start(3, gathers.at[2])

    total = half_step(
        1, 3, gathers.at[2], copies, gains2_ref, ("gate2", "up2", "down2"), gate2, up2, down2
    )
    mixed_out_ref[...] = (gathers[2, me].astype(F32) + 0.5 * total).astype(BF16)
    for copy in part_copies:
        copy.wait_send()
    store.wait()


def fused_call(mesh, *args):
    (
        tokens, lengths, state, gain_first, first_gate, first_up, first_down, gain_mix,
        query_weight, key_weight, value_weight, gating_weight, write_weight, forget_weight,
        forget_rate, out_weight, gain_second, second_gate, second_up, second_down,
    ) = args
    kv_size = mesh.shape["kv"]
    devices = kv_size * mesh.shape["tp"]
    rows, cols = tokens.shape
    channels = gain_first.shape[0]
    hidden_local = first_gate.shape[1]
    take = -(-hidden_local // 256) * 128
    phases = 2
    in_vmem = pl.BlockSpec(memory_space=pltpu.VMEM)
    in_smem = pl.BlockSpec(memory_space=pltpu.SMEM)
    in_any = pl.BlockSpec(memory_space=pl.ANY)
    dma = pltpu.SemaphoreType.DMA
    mixed_out, new_state = pl.pallas_call(
        functools.partial(fused_kernel, kv_size, channels),
        out_shape=(
            jax.ShapeDtypeStruct(tokens.shape, tokens.dtype),
            jax.ShapeDtypeStruct(state.shape, state.dtype),
        ),
        in_specs=[in_vmem, in_smem] + [in_vmem] * 4 + [in_any] * 14,
        out_specs=(in_vmem, in_any),
        scratch_shapes=[
            pltpu.VMEM((channels, take), BF16),
            pltpu.VMEM((channels, take), BF16),
            pltpu.VMEM((take, channels), BF16),
            pltpu.VMEM((channels, take), BF16),
            pltpu.VMEM((channels, take), BF16),
            pltpu.VMEM((take, channels), BF16),
            pltpu.VMEM((channels, 4 * cols), BF16),
            pltpu.VMEM(out_weight.shape, BF16),
            pltpu.VMEM((2 * HEADS, channels), BF16),
            pltpu.VMEM(state.shape[1:], F32),
            pltpu.VMEM(state.shape[1:], BF16),
            pltpu.VMEM(state.shape[1:], BF16),
            pltpu.VMEM(state.shape[1:], F32),
            pltpu.VMEM((rows, take), F32),
            pltpu.VMEM((rows, take), F32),
            pltpu.VMEM((rows, 4 * cols), F32),
            pltpu.VMEM((rows, 2 * HEADS), F32),
            pltpu.VMEM((3, devices, rows, cols), BF16),
            pltpu.VMEM((devices, BLK, HEADS * HEAD), BF16),
            pltpu.VMEM((phases, kv_size, rows, cols), F32),
            pltpu.VMEM((phases, kv_size, rows, cols), F32),
            pltpu.VMEM((phases, kv_size, rows, cols), BF16),
            pltpu.VMEM((phases, kv_size, rows, cols), BF16),
            pltpu.VMEM((devices, BLK, 4 * cols), BF16),
            pltpu.VMEM((devices, BLK, 4 * cols), BF16),
            dma((14,)),
            dma((4, 2 * kv_size)),
            dma((4, 2 * kv_size)),
            dma((phases, kv_size)),
            dma((phases, kv_size)),
            dma((phases, kv_size)),
            dma((phases, kv_size)),
            dma((devices,)),
            dma((devices,)),
            dma,
        ],
        compiler_params=pltpu.CompilerParams(
            collective_id=0, has_side_effects=True, vmem_limit_bytes=VMEM_LIMIT
        ),
    )(
        tokens, lengths, gain_first.reshape(1, -1), gain_mix.reshape(1, -1),
        gain_second.reshape(1, -1), forget_rate.reshape(1, -1), state,
        first_gate, first_up, first_down, query_weight, key_weight, value_weight,
        gating_weight, write_weight.T, forget_weight.T, out_weight, second_gate, second_up,
        second_down,
    )
    return hand_out(mixed_out, new_state)


def hand_out_kernel(mixed_ref, state_hbm, mixed_out_ref, state_out_hbm, held, in_sems, out_sems):
    heads = held.shape[0]
    count = in_sems.shape[0]
    step = heads // count
    takes, puts = [], []
    for i in range(count):
        at = pl.ds(i * step, step)
        takes.append(pltpu.make_async_copy(state_hbm.at[0, at], held.at[at], in_sems.at[i]))
        puts.append(pltpu.make_async_copy(held.at[at], state_out_hbm.at[0, at], out_sems.at[i]))
        takes[i].start()
    mixed_out_ref[...] = mixed_ref[...]
    for i in range(count):
        takes[i].wait()
        puts[i].start()
    for put in puts:
        put.wait()


def hand_out(mixed_out, new_state):
    in_vmem = pl.BlockSpec(memory_space=pltpu.VMEM)
    in_any = pl.BlockSpec(memory_space=pl.ANY)
    return pl.pallas_call(
        hand_out_kernel,
        out_shape=(
            jax.ShapeDtypeStruct(mixed_out.shape, mixed_out.dtype),
            jax.ShapeDtypeStruct(new_state.shape, new_state.dtype),
        ),
        in_specs=[in_vmem, in_any],
        out_specs=(in_vmem, in_any),
        scratch_shapes=[
            pltpu.VMEM(new_state.shape[1:], new_state.dtype),
            pltpu.SemaphoreType.DMA((4,)),
            pltpu.SemaphoreType.DMA((4,)),
        ],
        compiler_params=pltpu.CompilerParams(vmem_limit_bytes=VMEM_LIMIT),
    )(mixed_out, new_state)


def fits_fused(mesh, args):
    tokens, lengths, state, first_gate = args[0], args[1], args[2], args[4]
    rows, cols = tokens.shape
    devices = mesh.shape["kv"] * mesh.shape["tp"]
    return (
        mesh.shape["tp"] == 2
        and mesh.shape["kv"] & (mesh.shape["kv"] - 1) == 0
        and lengths.shape[0] == 1
        and rows == devices * BLK
        and cols % 256 == 0
        and first_gate.shape[1] % 128 == 0
        and state.shape[1:] == (HEADS, HEAD, HEAD)
    )


def solution(mesh):
    in_specs = (
        P("dp", ("kv", "tp")),
        P(("dp", "kv", "tp")),
        P(("dp", "kv", "tp"), None, None, None),
        P(),
        P(None, "kv"),
        P(None, "kv"),
        P("kv", None),
        P(),
        P(None, ("kv", "tp")),
        P(None, ("kv", "tp")),
        P(None, ("kv", "tp")),
        P(None, ("kv", "tp")),
        P(),
        P(),
        P(),
        P(None, ("kv", "tp")),
        P(),
        P(None, "kv"),
        P(None, "kv"),
        P("kv", None),
    )
    out_specs = (P("dp", ("kv", "tp")), P(("dp", "kv", "tp"), None, None, None))

    def body(*args):
        if fits_fused(mesh, args):
            return fused_call(mesh, *args)
        return per_device(*args)

    return jax.shard_map(
        body, mesh=mesh, in_specs=in_specs, out_specs=out_specs, check_vma=False
    )
```

```python
import functools
import math

import jax
import jax.numpy as jnp
from jax import lax
from jax.experimental import pallas as pl
from jax.experimental.pallas import tpu as pltpu
from jax.sharding import PartitionSpec as P

HEADS = 16
HEAD = 128
BLK = 8


EPSILON = 1e-06


def fold_step(gain, gate_cols, up_cols, portion):
    values = portion.astype(jnp.float32)
    scaled = (values * gain).astype(jnp.bfloat16)
    gate_acc = jnp.dot(scaled, gate_cols, preferred_element_type=jnp.float32)
    up_acc = jnp.dot(scaled, up_cols, preferred_element_type=jnp.float32)
    squares = jnp.sum(values * values, axis=1)
    return (gate_acc, up_acc, squares)


def finish_units(gate_acc, up_acc, squares, channels, down_rows):
    row_scale = lax.rsqrt(squares / channels + EPSILON)[:, None]
    hidden = (jax.nn.silu(gate_acc * row_scale) * (up_acc * row_scale)).astype(jnp.bfloat16)
    return jnp.dot(hidden, down_rows, preferred_element_type=jnp.float32)


def feed_forward(hidden_in, gain, w_gate, w_up, w_down):
    channels = gain.shape[0]
    paired = lax.all_to_all(hidden_in, "tp", split_axis=0, concat_axis=1, tiled=True)
    gate_acc, up_acc, squares = fold_step(
        gain, w_gate, w_up, lax.all_gather(paired, "kv", axis=1, tiled=True)
    )
    ffn_term = finish_units(gate_acc, up_acc, squares, channels, w_down)
    partial_value = lax.psum_scatter(ffn_term, "kv", scatter_dimension=1, tiled=True)
    summed = lax.all_to_all(partial_value, "tp", split_axis=1, concat_axis=0, tiled=True)
    return (hidden_in.astype(jnp.float32) + 0.5 * summed).astype(jnp.bfloat16)


def delta_block(query, key_in, value, gating, write_pre, forget_pre, rates, live, state):
    seq_count, block_len, head_count, head_size = query.shape
    precise = lax.Precision.HIGHEST
    query_unit = (
        query
        * lax.rsqrt(jnp.sum(query * query, axis=-1, keepdims=True) + EPSILON)
        / math.sqrt(head_size)
    )
    key_unit = key_in * lax.rsqrt(jnp.sum(key_in * key_in, axis=-1, keepdims=True) + EPSILON)
    live_rows = live[:, :, None]
    write_gate = jax.nn.sigmoid(write_pre) * live_rows
    forget = -jnp.exp(rates)[None, None, :] * jax.nn.softplus(forget_pre) * live_rows
    cumulative = jnp.cumsum(forget, axis=1)
    cum_heads = jnp.transpose(cumulative, (0, 2, 1))
    positions = jnp.arange(block_len)
    causal = positions[:, None] >= positions[None, :]
    strict = positions[:, None] > positions[None, :]
    differ = jnp.minimum(cum_heads[:, :, :, None] - cum_heads[:, :, None, :], 0.0)
    decay_mat = jnp.where(causal, jnp.exp(differ), 0.0)
    key_dots = jnp.einsum("sthd,suhd->shtu", key_unit, key_unit, precision=precise)
    write_heads = jnp.transpose(write_gate, (0, 2, 1))
    strict_part = jnp.where(strict, write_heads[:, :, :, None] * decay_mat * key_dots, 0.0)
    identity = jnp.eye(block_len, dtype=jnp.float32)
    squared = jnp.einsum("shtu,shuv->shtv", strict_part, strict_part, precision=precise)
    fourth = jnp.einsum("shtu,shuv->shtv", squared, squared, precision=precise)
    inverse = jnp.einsum(
        "shtu,shuv->shtv", identity - strict_part, identity + squared, precision=precise
    )
    inverse = jnp.einsum("shtu,shuv->shtv", inverse, identity + fourth, precision=precise)
    growth = jnp.exp(cumulative)
    target = jnp.einsum(
        "shtu,suhv->sthv", inverse, write_gate[..., None] * value, precision=precise
    )
    key_mix = jnp.einsum(
        "shtu,suhk->sthk", inverse, (write_gate * growth)[..., None] * key_unit, precision=precise
    )
    update = target - jnp.einsum("sthk,shkv->sthv", key_mix, state, precision=precise)
    scores = jnp.einsum("sthd,suhd->shtu", query_unit, key_unit, precision=precise) * decay_mat
    attend = jnp.einsum("sthk,shkv->sthv", query_unit * growth[..., None], state, precision=precise)
    attend = attend + jnp.einsum("shtu,suhv->sthv", scores, update, precision=precise)
    final_cum = cumulative[:, -1:, :]
    fading = jnp.exp(final_cum - cumulative)
    new_state = jnp.exp(final_cum[:, 0, :])[:, :, None, None] * state
    new_state = new_state + jnp.einsum(
        "sthk,sthv->shkv", key_unit * fading[..., None], update, precision=precise
    )
    normed = attend * lax.rsqrt(jnp.mean(attend * attend, axis=-1, keepdims=True) + EPSILON)
    normed = normed * jax.nn.silu(gating) * live[:, :, None, None]
    mixed_heads = normed.reshape(seq_count * block_len, head_count * head_size).astype(jnp.bfloat16)
    return (mixed_heads, new_state)


def per_device(
    tokens,
    lengths,
    state,
    gain_first,
    first_gate,
    first_up,
    first_down,
    gain_mix,
    query_weight,
    key_weight,
    value_weight,
    gating_weight,
    write_weight,
    forget_weight,
    forget_rate,
    out_weight,
    gain_second,
    second_gate,
    second_up,
    second_down,
):
    after_first = feed_forward(tokens, gain_first, first_gate, first_up, first_down)
    seq_count = lengths.shape[0]
    own_count = seq_count * BLK
    whole_rows = lax.all_gather(after_first, ("kv", "tp"), axis=1, tiled=True)
    scaled_all = (whole_rows.astype(jnp.float32) * gain_mix).astype(jnp.bfloat16)
    stacked = jnp.stack(
        [
            jnp.dot(scaled_all, matrix, preferred_element_type=jnp.float32)
            for matrix in (query_weight, key_weight, value_weight, gating_weight)
        ]
    )
    owned = lax.all_to_all(
        stacked.astype(jnp.bfloat16), ("kv", "tp"), split_axis=1, concat_axis=2, tiled=True
    ).astype(stacked.dtype)
    row_start = lax.axis_index(("kv", "tp")) * own_count
    own_values = lax.dynamic_slice_in_dim(whole_rows, row_start, own_count, 0).astype(jnp.float32)
    own_scaled = lax.dynamic_slice_in_dim(scaled_all, row_start, own_count, 0)
    mix_scale = lax.rsqrt(jnp.mean(own_values * own_values, axis=1, keepdims=True) + EPSILON)
    query = (owned[0] * mix_scale).reshape(seq_count, BLK, HEADS, HEAD)
    key_in = (owned[1] * mix_scale).reshape(seq_count, BLK, HEADS, HEAD)
    value = (owned[2] * mix_scale).reshape(seq_count, BLK, HEADS, HEAD)
    gating = (owned[3] * mix_scale).reshape(seq_count, BLK, HEADS, HEAD)
    write_pre = (
        jnp.dot(own_scaled, write_weight, preferred_element_type=jnp.float32) * mix_scale
    ).reshape(seq_count, BLK, HEADS)
    forget_pre = (
        jnp.dot(own_scaled, forget_weight, preferred_element_type=jnp.float32) * mix_scale
    ).reshape(seq_count, BLK, HEADS)
    positions = jnp.arange(BLK, dtype=jnp.int32)
    live = (positions[None, :] < lengths[:, None]).astype(jnp.float32)
    mixed_heads, new_state = delta_block(
        query, key_in, value, gating, write_pre, forget_pre, forget_rate, live, state
    )
    half_cols = mixed_heads.shape[1] // 2
    portion = lax.all_gather(mixed_heads, ("kv", "tp"), axis=0, tiled=True)
    first_half = jnp.dot(
        portion[:, :half_cols], out_weight[:half_cols], preferred_element_type=jnp.float32
    ).astype(jnp.bfloat16)
    second_half = jnp.dot(
        portion[:, half_cols:], out_weight[half_cols:], preferred_element_type=jnp.float32
    ).astype(jnp.bfloat16)
    first_half, second_half = lax.optimization_barrier((first_half, second_half))
    mixed_sum = first_half.astype(jnp.float32) + second_half.astype(jnp.float32)
    after_mix = (after_first.astype(jnp.float32) + mixed_sum).astype(jnp.bfloat16)
    mixed_out = feed_forward(after_mix, gain_second, second_gate, second_up, second_down)
    return (mixed_out, new_state)


F32 = jnp.float32
BF16 = jnp.bfloat16
MESH = pl.DeviceIdType.MESH
VMEM_LIMIT = 60 * 1024 * 1024


def fused_kernel(
    kv_size,
    channels,
    tokens_hbm,
    lengths_ref,
    gains1_hbm,
    gains_mix_hbm,
    gains2_hbm,
    rates_hbm,
    state_hbm,
    gate1_hbm,
    up1_hbm,
    down1_hbm,
    query_hbm,
    key_hbm,
    value_hbm,
    gating_hbm,
    write_hbm,
    forget_hbm,
    out_hbm,
    gate2_hbm,
    up2_hbm,
    down2_hbm,
    mixed_out_ref,
    new_state_hbm,
    gate1,
    up1,
    down1,
    gate2,
    up2,
    down2,
    proj,
    out_w,
    small_w,
    state,
    state_high,
    state_low,
    gains1_ref,
    gains_mix_ref,
    gains2_ref,
    rates_ref,
    state_out,
    gate_acc,
    up_acc,
    proj_acc,
    small_acc,
    gathers,
    heads_all,
    pair_send,
    pair_recv,
    red_send,
    red_recv,
    part_send,
    part_recv,
    load_sems,
    gather_send_sems,
    gather_recv_sems,
    pair_send_sems,
    pair_recv_sems,
    red_send_sems,
    red_recv_sems,
    part_send_sems,
    part_recv_sems,
    store_sem,
):
    kv = lax.axis_index("kv")
    tp = lax.axis_index("tp")
    devices = 2 * kv_size
    me = kv * 2 + tp
    rows, cols = tokens_hbm.shape
    take = gate1.shape[1]
    hidden_local = gate1_hbm.shape[1]
    lead = hidden_local - take
    overlap = 2 * take - hidden_local
    first_col = pl.multiple_of(tp * lead, 128)

    def load(index, src, dst):
        return pltpu.make_async_copy(src, dst, load_sems.at[index])

    cut = pl.ds(first_col, take)
    loads = {
        "gate1": load(0, gate1_hbm.at[:, cut], gate1),
        "up1": load(1, up1_hbm.at[:, cut], up1),
        "down1": load(2, down1_hbm.at[cut, :], down1),
        "query": load(3, query_hbm, proj.at[:, 0:cols]),
        "key": load(4, key_hbm, proj.at[:, cols : 2 * cols]),
        "value": load(5, value_hbm, proj.at[:, 2 * cols : 3 * cols]),
        "gating": load(6, gating_hbm, proj.at[:, 3 * cols : 4 * cols]),
        "write": load(7, write_hbm, small_w.at[0:HEADS]),
        "forget": load(8, forget_hbm, small_w.at[HEADS : 2 * HEADS]),
        "state": load(9, state_hbm.at[0], state),
        "out": load(10, out_hbm, out_w),
        "gate2": load(11, gate2_hbm.at[:, cut], gate2),
        "up2": load(12, up2_hbm.at[:, cut], up2),
        "down2": load(13, down2_hbm.at[cut, :], down2),
        "tokens": load(14, tokens_hbm, gathers.at[0, me]),
        "gains1": load(15, gains1_hbm, gains1_ref),
        "gains_mix": load(16, gains_mix_hbm, gains_mix_ref),
        "gains2": load(17, gains2_hbm, gains2_ref),
        "rates": load(18, rates_hbm, rates_ref),
    }
    small = ("tokens", "gains1", "gains_mix", "gains2", "rates")
    for name in small + ("gate1", "up1", "down1"):
        loads[name].start()

    def remote(src, dst, send_sem, recv_sem, to_kv, to_tp):
        return pltpu.make_async_remote_copy(
            src_ref=src,
            dst_ref=dst,
            send_sem=send_sem,
            recv_sem=recv_sem,
            device_id={"kv": to_kv, "tp": to_tp},
            device_id_type=MESH,
        )

    barrier = pltpu.get_barrier_semaphore()
    for off in range(1, devices):
        peer = lax.rem(me + off, devices)
        pl.semaphore_signal(
            barrier,
            inc=1,
            device_id={"kv": peer // 2, "tp": lax.rem(peer, 2)},
            device_id_type=MESH,
        )
    pl.semaphore_wait(barrier, devices - 1)

    sent = []

    def swapped(off):
        chip, bit = kv, 1
        while bit < kv_size:
            if off & bit:
                chip = chip + bit - 2 * bit * lax.rem(kv // bit, 2)
            bit *= 2
        return chip

    def gather_start(phase, buf):
        copies = {}
        for off in list(range(kv_size - 1, 0, -1)) + [0]:
            copies[off] = remote(
                buf.at[me],
                buf.at[me],
                gather_send_sems.at[phase, off],
                gather_recv_sems.at[phase, off],
                swapped(off),
                1 - tp,
            )
            copies[off].start()
        return copies

    def gather_finish(phase, buf, copies, use=lambda slot, first: None):
        use(me, True)
        copies[0].wait_recv()
        use(kv * 2 + 1 - tp, False)
        forwards = {}
        for off in range(1, kv_size):
            copies[off].wait_recv()
            slot = swapped(off) * 2 + 1 - tp
            forwards[off] = remote(
                buf.at[slot],
                buf.at[slot],
                gather_send_sems.at[phase, kv_size - 1 + off],
                gather_recv_sems.at[phase, kv_size - 1 + off],
                kv,
                1 - tp,
            )
            forwards[off].start()
        for off in range(1, kv_size):
            use(swapped(off) * 2 + 1 - tp, False)
        for off in range(1, kv_size):
            forwards[off].wait_recv()
            use(swapped(off) * 2 + tp, False)
        sent.extend(copies.values())
        sent.extend(forwards.values())

    def multiply(buf, gain_ref, products):
        squares = [jnp.zeros((rows, 1), F32)]

        def use(slot, first):
            at = pl.ds(pl.multiple_of(slot * cols, cols), cols)
            values = buf[slot].astype(F32)
            squares[0] = squares[0] + jnp.sum(values * values, axis=1, keepdims=True)
            scaled = (values * gain_ref[:, at]).astype(BF16)
            for acc, weight, across in products:
                if across:
                    term = lax.dot_general(
                        scaled,
                        weight[:, at],
                        (((1,), (1,)), ((), ())),
                        preferred_element_type=F32,
                    )
                else:
                    term = jnp.dot(scaled, weight[at, :], preferred_element_type=F32)
                if first:
                    acc[...] = term
                else:
                    acc[...] += term

        return squares, use

    def inverse_rms(squares):
        return lax.rsqrt(squares[0] / channels + EPSILON)

    def half_step(phase, at, buf, copies, gain_ref, names, gate_w, up_w, down_w):
        loads[names[0]].wait()
        loads[names[1]].wait()
        squares, use = multiply(buf, gain_ref, ((gate_acc, gate_w, False), (up_acc, up_w, False)))
        gather_finish(at, buf, copies, use)
        row_scale = inverse_rms(squares)
        gate = gate_acc[...] * row_scale
        up = up_acc[...] * row_scale
        column = lax.broadcasted_iota(jnp.int32, (rows, take), 1)
        hidden = jnp.where(column >= tp * overlap, jax.nn.silu(gate) * up, 0.0).astype(BF16)
        loads[names[2]].wait()

        def columns_of(chip, core):
            at = pl.multiple_of((chip * 2 + core) * cols, cols)
            return jnp.dot(hidden, down_w[:, pl.ds(at, cols)], preferred_element_type=F32)

        order = list(range(kv_size - 1, -1, -1))
        pair_copies = []
        for off in order:
            pair_send[phase, off] = columns_of(swapped(off), tp if off else 1 - tp)
            copy = remote(
                pair_send.at[phase, off],
                pair_recv.at[phase, off],
                pair_send_sems.at[phase, off],
                pair_recv_sems.at[phase, off],
                kv,
                1 - tp,
            )
            copy.start()
            pair_copies.append(copy)
        red_copies = []
        total = None
        for position, off in enumerate(order):
            term = columns_of(swapped(off), 1 - tp if off else tp)
            pair_copies[position].wait_recv()
            term = term + pair_recv[phase, off]
            if off == 0:
                total = term
                continue
            red_send[phase, off] = term.astype(BF16)
            copy = remote(
                red_send.at[phase, off],
                red_recv.at[phase, off],
                red_send_sems.at[phase, off],
                red_recv_sems.at[phase, off],
                swapped(off),
                1 - tp,
            )
            copy.start()
            red_copies.append(copy)
        for copy in red_copies[::-1]:
            copy.wait_recv()
        for off in range(1, kv_size):
            total = total + red_recv[phase, off].astype(F32)
        sent.extend(pair_copies + red_copies)
        return total

    for name in small:
        loads[name].wait()
    copies = gather_start(0, gathers.at[0])
    for name in ("query", "key", "value", "gating", "write", "forget", "state", "out"):
        loads[name].start()
    for name in ("gate2", "up2", "down2"):
        loads[name].start()
    total = half_step(
        0, 0, gathers.at[0], copies, gains1_ref, ("gate1", "up1", "down1"), gate1, up1, down1
    )
    after_first = (gathers[0, me].astype(F32) + 0.5 * total).astype(BF16)
    gathers[1, me] = after_first
    copies = gather_start(1, gathers.at[1])

    loads["state"].wait()
    for head in range(HEADS):
        high = state[head].astype(BF16)
        state_high[head] = high
        state_low[head] = (state[head] - high.astype(F32)).astype(BF16)
    for name in ("query", "key", "value", "gating", "write", "forget"):
        loads[name].wait()
    squares, use = multiply(
        gathers.at[1], gains_mix_ref, ((proj_acc, proj, False), (small_acc, small_w, True))
    )
    gather_finish(1, gathers.at[1], copies, use)
    mix_scale = inverse_rms(squares)
    part_send[...] = (proj_acc[...] * mix_scale).reshape(devices, BLK, 4 * cols).astype(BF16)
    part_copies = []
    for off in range(1, devices):
        peer = lax.rem(me + off, devices)
        copy = remote(
            part_send.at[peer],
            part_recv.at[me],
            part_send_sems.at[off],
            part_recv_sems.at[off],
            peer // 2,
            lax.rem(peer, 2),
        )
        copy.start()
        part_copies.append(copy)
    part_recv[me] = part_send[me]
    small_acc[...] = small_acc[...] * mix_scale
    own = pl.ds(pl.multiple_of(me * BLK, BLK), BLK)
    write_pre = small_acc[own, 0:HEADS]
    forget_pre = small_acc[own, HEADS : 2 * HEADS]

    size = HEADS * BLK
    row = lax.broadcasted_iota(jnp.int32, (size, size), 0)
    col = lax.broadcasted_iota(jnp.int32, (size, size), 1)
    same = (row // BLK) == (col // BLK)
    causal = same & (row >= col)
    strict = same & (row > col)
    diagonal = row == col
    identity = jnp.where(diagonal, 1.0, 0.0)
    head_row = lax.broadcasted_iota(jnp.int32, (size, HEADS), 0) // BLK
    head_col = lax.broadcasted_iota(jnp.int32, (size, HEADS), 1)
    pick = head_row == head_col

    def as_column(block):
        return jnp.sum(jnp.where(pick, block, 0.0), axis=1, keepdims=True)

    def to_row(column):
        return jnp.sum(jnp.where(diagonal, column, 0.0), axis=0, keepdims=True)

    token_at = lax.rem(lax.broadcasted_iota(jnp.int32, (size, 1), 0), BLK)
    live = jnp.where(token_at < lengths_ref[0], 1.0, 0.0)
    write_col = as_column(jnp.concatenate([write_pre] * HEADS, axis=0))
    forget_col = as_column(jnp.concatenate([forget_pre] * HEADS, axis=0))
    rate_col = as_column(jnp.broadcast_to(rates_ref[...], (size, HEADS)))
    write_gate = jax.nn.sigmoid(write_col) * live
    softplus = jnp.maximum(forget_col, 0.0) + jnp.log1p(jnp.exp(-jnp.abs(forget_col)))
    forget = -jnp.exp(rate_col) * softplus * live
    forget_row = to_row(forget)
    cumulative = jnp.sum(jnp.where(causal, forget_row, 0.0), axis=1, keepdims=True)
    final = jnp.sum(jnp.where(same, forget_row, 0.0), axis=1, keepdims=True)
    decay = jnp.where(causal, jnp.exp(jnp.minimum(cumulative - to_row(cumulative), 0.0)), 0.0)
    growth = jnp.exp(cumulative)
    fading = jnp.exp(final - cumulative)
    shrink = jnp.exp(final)

    for copy in part_copies:
        copy.wait_recv()

    def by_head(index):
        pieces = []
        for j in range(devices):
            block = part_recv[j, :, index * cols : (index + 1) * cols].astype(F32)
            for at in range(0, cols, HEAD):
                pieces.append(block[:, at : at + HEAD])
        return jnp.concatenate(pieces, axis=0)

    def cut_terms(a):
        high = a.astype(BF16).astype(F32)
        return high, a - high

    def dot(a, b, across=False):
        high_a, low_a = cut_terms(a)
        high_b, low_b = cut_terms(b)
        axis = 1 if across else 0
        left = jnp.concatenate([high_a, high_a, low_a], axis=1).astype(BF16)
        right = jnp.concatenate([high_b, low_b, high_b], axis=axis).astype(BF16)
        return lax.dot_general(
            left, right, (((1,), (axis,)), ((), ())), preferred_element_type=F32
        )

    query, key_in, value, gating = (by_head(index) for index in range(4))
    query_unit = (
        query
        * lax.rsqrt(jnp.sum(query * query, axis=1, keepdims=True) + EPSILON)
        * (1.0 / math.sqrt(HEAD))
    )
    key_unit = key_in * lax.rsqrt(jnp.sum(key_in * key_in, axis=1, keepdims=True) + EPSILON)
    products = dot(jnp.concatenate([key_unit, query_unit], axis=0), key_unit, True)
    lower = products[:size]
    lower = jnp.where(strict, write_gate * decay * lower, 0.0)
    squared = dot(lower, lower)
    fourth = dot(squared, squared)
    inverse = dot(identity - lower, identity + squared)
    inverse = dot(inverse, identity + fourth)
    key_grown = (write_gate * growth) * key_unit
    query_grown = query_unit * growth
    scores = products[size:] * decay

    key_terms, query_terms = [], []
    for head in range(HEADS):
        at = slice(head * BLK, (head + 1) * BLK)
        high, low = cut_terms(jnp.concatenate([key_grown[at], query_grown[at]], axis=0))
        both = jnp.concatenate([high, low], axis=0).astype(BF16)
        result = jnp.dot(both, state_high[head], preferred_element_type=F32)
        result = result[: 2 * BLK] + result[2 * BLK :]
        result = result + jnp.dot(
            both[: 2 * BLK], state_low[head], preferred_element_type=F32
        )
        key_terms.append(result[:BLK])
        query_terms.append(result[BLK:])
    update = dot(inverse, write_gate * value - jnp.concatenate(key_terms, axis=0))
    attend = jnp.concatenate(query_terms, axis=0) + dot(scores, update)
    normed = attend * lax.rsqrt(jnp.mean(attend * attend, axis=1, keepdims=True) + EPSILON)
    normed = normed * jax.nn.silu(gating) * live
    heads_all[me] = jnp.concatenate(
        [normed[head * BLK : (head + 1) * BLK] for head in range(HEADS)], axis=1
    ).astype(BF16)
    copies = gather_start(2, heads_all)
    faded = key_unit * fading
    for head in range(HEADS):
        at = slice(head * BLK, (head + 1) * BLK)
        key_high, key_low = cut_terms(faded[at])
        value_high, value_low = cut_terms(update[at])
        outer = lax.dot_general(
            jnp.concatenate([key_high, key_high, key_low], axis=0).astype(BF16),
            jnp.concatenate([value_high, value_low, value_high], axis=0).astype(BF16),
            (((0,), (0,)), ((), ())),
            preferred_element_type=F32,
        )
        state_out[head] = shrink[head * BLK : head * BLK + 1] * state[head] + outer
    store = pltpu.make_async_copy(state_out, new_state_hbm.at[0], store_sem)
    store.start()
    gather_finish(2, heads_all, copies)

    mixed = heads_all[...].astype(F32).reshape(rows, HEADS * HEAD).astype(BF16)
    loads["out"].wait()
    half = HEADS * HEAD // 2
    first = jnp.dot(mixed[:, :half], out_w[:half], preferred_element_type=F32).astype(BF16)
    second = jnp.dot(mixed[:, half:], out_w[half:], preferred_element_type=F32).astype(BF16)
    residual = gathers[1, me].astype(F32)
    after_mix = (residual + (first.astype(F32) + second.astype(F32))).astype(BF16)
    gathers[2, me] = after_mix
    copies = gather_start(3, gathers.at[2])

    total = half_step(
        1, 3, gathers.at[2], copies, gains2_ref, ("gate2", "up2", "down2"), gate2, up2, down2
    )
    mixed_out_ref[...] = (gathers[2, me].astype(F32) + 0.5 * total).astype(BF16)
    for copy in part_copies + sent:
        copy.wait_send()
    store.wait()


def fused_call(mesh, *args):
    (
        tokens, lengths, state, gain_first, first_gate, first_up, first_down, gain_mix,
        query_weight, key_weight, value_weight, gating_weight, write_weight, forget_weight,
        forget_rate, out_weight, gain_second, second_gate, second_up, second_down,
    ) = args
    kv_size = mesh.shape["kv"]
    devices = kv_size * mesh.shape["tp"]
    rows, cols = tokens.shape
    channels = gain_first.shape[0]
    hidden_local = first_gate.shape[1]
    take = -(-hidden_local // 256) * 128
    phases = 2
    in_vmem = pl.BlockSpec(memory_space=pltpu.VMEM)
    in_smem = pl.BlockSpec(memory_space=pltpu.SMEM)
    in_any = pl.BlockSpec(memory_space=pl.ANY)
    dma = pltpu.SemaphoreType.DMA
    mixed_out, new_state = pl.pallas_call(
        functools.partial(fused_kernel, kv_size, channels),
        out_shape=(
            jax.ShapeDtypeStruct(tokens.shape, tokens.dtype),
            jax.ShapeDtypeStruct(state.shape, state.dtype),
        ),
        in_specs=[in_any, in_smem] + [in_any] * 18,
        out_specs=(in_vmem, in_any),
        scratch_shapes=[
            pltpu.VMEM((channels, take), BF16),
            pltpu.VMEM((channels, take), BF16),
            pltpu.VMEM((take, channels), BF16),
            pltpu.VMEM((channels, take), BF16),
            pltpu.VMEM((channels, take), BF16),
            pltpu.VMEM((take, channels), BF16),
            pltpu.VMEM((channels, 4 * cols), BF16),
            pltpu.VMEM(out_weight.shape, BF16),
            pltpu.VMEM((2 * HEADS, channels), BF16),
            pltpu.VMEM(state.shape[1:], F32),
            pltpu.VMEM(state.shape[1:], BF16),
            pltpu.VMEM(state.shape[1:], BF16),
            pltpu.VMEM((1, channels), F32),
            pltpu.VMEM((1, channels), F32),
            pltpu.VMEM((1, channels), F32),
            pltpu.VMEM((1, HEADS), F32),
            pltpu.VMEM(state.shape[1:], F32),
            pltpu.VMEM((rows, take), F32),
            pltpu.VMEM((rows, take), F32),
            pltpu.VMEM((rows, 4 * cols), F32),
            pltpu.VMEM((rows, 2 * HEADS), F32),
            pltpu.VMEM((3, devices, rows, cols), BF16),
            pltpu.VMEM((devices, BLK, HEADS * HEAD), BF16),
            pltpu.VMEM((phases, kv_size, rows, cols), F32),
            pltpu.VMEM((phases, kv_size, rows, cols), F32),
            pltpu.VMEM((phases, kv_size, rows, cols), BF16),
            pltpu.VMEM((phases, kv_size, rows, cols), BF16),
            pltpu.VMEM((devices, BLK, 4 * cols), BF16),
            pltpu.VMEM((devices, BLK, 4 * cols), BF16),
            dma((19,)),
            dma((4, 2 * kv_size)),
            dma((4, 2 * kv_size)),
            dma((phases, kv_size)),
            dma((phases, kv_size)),
            dma((phases, kv_size)),
            dma((phases, kv_size)),
            dma((devices,)),
            dma((devices,)),
            dma,
        ],
        compiler_params=pltpu.CompilerParams(
            collective_id=0, has_side_effects=True, vmem_limit_bytes=VMEM_LIMIT
        ),
    )(
        tokens, lengths, gain_first.reshape(1, -1), gain_mix.reshape(1, -1),
        gain_second.reshape(1, -1), forget_rate.reshape(1, -1), state,
        first_gate, first_up, first_down, query_weight, key_weight, value_weight,
        gating_weight, write_weight.T, forget_weight.T, out_weight, second_gate, second_up,
        second_down,
    )
    return hand_out(mixed_out, new_state)


def hand_out_kernel(mixed_hbm, state_hbm, mixed_out_hbm, state_out_hbm, mixed, held, in_sems, out_sems):
    heads = held.shape[0]
    count = in_sems.shape[0] - 1
    step = heads // count
    takes = [pltpu.make_async_copy(mixed_hbm, mixed, in_sems.at[count])]
    puts = [pltpu.make_async_copy(mixed, mixed_out_hbm, out_sems.at[count])]
    for i in range(count):
        at = pl.ds(i * step, step)
        takes.append(pltpu.make_async_copy(state_hbm.at[0, at], held.at[at], in_sems.at[i]))
        puts.append(pltpu.make_async_copy(held.at[at], state_out_hbm.at[0, at], out_sems.at[i]))
    for take in takes:
        take.start()
    for take, put in zip(takes, puts):
        take.wait()
        put.start()
    for put in puts:
        put.wait()


def hand_out(mixed_out, new_state):
    in_any = pl.BlockSpec(memory_space=pl.ANY)
    return pl.pallas_call(
        hand_out_kernel,
        out_shape=(
            jax.ShapeDtypeStruct(mixed_out.shape, mixed_out.dtype),
            jax.ShapeDtypeStruct(new_state.shape, new_state.dtype),
        ),
        in_specs=[in_any, in_any],
        out_specs=(in_any, in_any),
        scratch_shapes=[
            pltpu.VMEM(mixed_out.shape, mixed_out.dtype),
            pltpu.VMEM(new_state.shape[1:], new_state.dtype),
            pltpu.SemaphoreType.DMA((5,)),
            pltpu.SemaphoreType.DMA((5,)),
        ],
        compiler_params=pltpu.CompilerParams(vmem_limit_bytes=VMEM_LIMIT),
    )(mixed_out, new_state)


def fits_fused(mesh, args):
    tokens, lengths, state, first_gate = args[0], args[1], args[2], args[4]
    rows, cols = tokens.shape
    devices = mesh.shape["kv"] * mesh.shape["tp"]
    return (
        mesh.shape["tp"] == 2
        and mesh.shape["kv"] & (mesh.shape["kv"] - 1) == 0
        and lengths.shape[0] == 1
        and rows == devices * BLK
        and cols % 256 == 0
        and first_gate.shape[1] % 128 == 0
        and state.shape[1:] == (HEADS, HEAD, HEAD)
    )


def solution(mesh):
    in_specs = (
        P("dp", ("kv", "tp")),
        P(("dp", "kv", "tp")),
        P(("dp", "kv", "tp"), None, None, None),
        P(),
        P(None, "kv"),
        P(None, "kv"),
        P("kv", None),
        P(),
        P(None, ("kv", "tp")),
        P(None, ("kv", "tp")),
        P(None, ("kv", "tp")),
        P(None, ("kv", "tp")),
        P(),
        P(),
        P(),
        P(None, ("kv", "tp")),
        P(),
        P(None, "kv"),
        P(None, "kv"),
        P("kv", None),
    )
    out_specs = (P("dp", ("kv", "tp")), P(("dp", "kv", "tp"), None, None, None))

    def body(*args):
        if fits_fused(mesh, args):
            return fused_call(mesh, *args)
        return per_device(*args)

    return jax.shard_map(
        body, mesh=mesh, in_specs=in_specs, out_specs=out_specs, check_vma=False
    )
```
